512 devices in a mesh: sp: 64 (over z, y), fs: 4 (over x), tp: 2 (over core).
Axes of the slice: x: 4, y: 8, z: 8, core: 2. Of those that a mesh axis runs over, the one named last changes fastest.
Arguments:
- tokens: bfloat16 [131072, 2048], P(('fs', 'sp', 'tp')), parts along dimension 0, may hold values from -60 to 60
- norm_gain: float32 [2048], replicated, may hold values from 0.1 to 1.9
- pool_in: bfloat16 [2048, 512], P('sp', 'tp'), may hold values from -0.125 to 0.125
- gate_in: bfloat16 [2048, 1024], P('sp', 'tp'), may hold values from -0.125 to 0.125
- value_in: bfloat16 [2048, 1024], P('sp', 'tp'), may hold values from -0.125 to 0.125
- pool_mix: bfloat16 [4, 128, 128], P('tp'), may hold values from -0.5 to 0.5
- averaging_factor: float32 [512], P('tp'), may hold values from 0.25 to 0.75
- conv_taps: float32 [4, 1024], P(None, 'tp'), may hold values from -3 to 3
- rate_mix: bfloat16 [16, 64, 64], P('tp'), may hold values from -0.75 to 0.75
- input_mix: bfloat16 [16, 64, 64], P('tp'), may hold values from -0.75 to 0.75
- log_rate: float32 [1024], P('tp'), may hold values from 1.5 to 16
- decay_shift: float32 [64, 32768], P(('fs', 'tp'), 'sp'), parts along dimension 0, may hold values from -1.1 to 0
- initial_state: float32 [4096], P(('fs', 'tp')), parts along dimension 0, may hold values from -6 to 6
- out_pool: bfloat16 [2048, 512], P('sp', 'tp'), may hold values from -0.15625 to 0.15625
- out_rnn: bfloat16 [2048, 1024], P('sp', 'tp'), may hold values from -0.15625 to 0.15625
Outputs:
- mixed: bfloat16 [131072, 2048], P(('fs', 'sp', 'tp')), parts along dimension 0
The draws below stay inside these ranges and needn't reach their ends.
There are 4 independent parts, one for each index of `fs`. The reference program is written for one: setup_inputs(seed, part) draws one part's arguments, and reference() takes and returns one part's arrays. A program takes and returns all parts, laid end to end along the dimension named above; an argument that names none is the same for every part. Nothing has to cross between parts.
All inputs are finite; a program needn't handle non-finite values.
Results may differ from the reference program's by a relative error of at most 0.012.
Values may be sent and summed in bfloat16 or wider, within the bound.
A program may use at most 64 MiB of HBM per device.

```python
import math
import jax
import jax.numpy as jnp
from jax import lax

D = 2048
POOL = 512
GROUPS = 4
GROUP_WIDTH = 128
LOOP_BRANCHES = 16
HEAD_DIM = 64
RNN = 1024
TAPS = 4
REACH = 16
TOK_DEV = 512
TOKEN_COUNT = 32768


def draw_tokens(key, part):
    derived_seed_list = jax.random.split(key, 3)
    row_scales = jnp.exp(jax.random.uniform(derived_seed_list[0], (TOKEN_COUNT, 1), jnp.float32, math.log(0.5), math.log(5.0)))
    column_scales = jnp.exp(jax.random.uniform(derived_seed_list[1], (1, D), jnp.float32, math.log(0.3), math.log(3.0)))
    entries = jax.random.truncated_normal(derived_seed_list[2], -4.0, 4.0, (TOKEN_COUNT, D), jnp.float32)
    return (entries * row_scales * column_scales).astype(jnp.bfloat16)


def draw_log_rate(key, part):
    derived_seed_list = jax.random.split(key, 3)
    chance = 0.5
    fast_heads = jax.random.bernoulli(derived_seed_list[0], chance, (LOOP_BRANCHES,))
    fast_rate = jax.random.uniform(derived_seed_list[1], (RNN,), jnp.float32, 2.0, 4.0) / TOK_DEV
    slow_rate = jax.random.uniform(derived_seed_list[2], (RNN,), jnp.float32, 0.04, 0.12) / TOKEN_COUNT
    per_channel = jnp.repeat(fast_heads, HEAD_DIM)
    step_rate = jnp.where(per_channel, fast_rate, slow_rate)
    return -jnp.log(jnp.expm1(step_rate))


def draw_decay_shift(key, part):
    derived_seed_list = jax.random.split(key, 3)
    blocks = TOKEN_COUNT // TOK_DEV
    block_level = jnp.exp(jax.random.uniform(derived_seed_list[0], (LOOP_BRANCHES, blocks), jnp.float32, math.log(0.1), math.log(2.0))) / TOKEN_COUNT
    steady_signal = -jnp.repeat(block_level, TOK_DEV, axis=1)
    cluster_indices = jax.random.randint(derived_seed_list[1], (LOOP_BRANCHES, 2, 1), 0, TOKEN_COUNT)
    loss_values = jax.random.uniform(derived_seed_list[2], (LOOP_BRANCHES, 2, 1), jnp.float32, 0.2, 0.4)
    match_tests = jnp.arange(TOKEN_COUNT, dtype=jnp.int32)[None, None, :] == cluster_indices
    spike_events = jnp.sum(jnp.where(match_tests, jnp.log1p(-loss_values), 0.0), axis=1)
    return steady_signal + spike_events


def shard_levels(key, shape, cuts, smallest, largest):
    level, own = 1.0, jax.random.fold_in(key, 6)
    for axis_at, parts in cuts:
        draws = jnp.exp(jax.random.uniform(jax.random.fold_in(own, axis_at), (parts,), jnp.float32, smallest / len(cuts), largest / len(cuts)))
        level = level * jnp.repeat(draws, shape[axis_at] // parts).reshape([-1 if axis == axis_at else 1 for axis in range(len(shape))])
    return level


def centred(own_key, shape, width, bound, cuts=(), kind=jnp.bfloat16):
    result = width * jax.random.normal(own_key, shape, jnp.float32)
    if cuts:
        result = result * shard_levels(own_key, shape, cuts, -0.22, 0.18)
    return jnp.clip(result, -bound, bound).astype(kind)


def setup_inputs(seed: int = 0, part: int = 0) -> dict:
    arg_keys = jax.random.split(jax.random.key(seed), 16)
    part_keys = jax.random.split(jax.random.fold_in(arg_keys[15], part), 16)
    tokens = draw_tokens(jax.random.fold_in(jax.random.fold_in(arg_keys[15], part), 71), part)
    norm_gain = jnp.clip(1.0 + 0.18 * jax.random.normal(arg_keys[1], (D,), jnp.float32), 0.1, 1.9)
    pool_in = centred(arg_keys[2], (D, POOL), D ** -0.5, 0.125, ((0, 64), (1, 2)))
    gate_in = centred(arg_keys[3], (D, RNN), D ** -0.5, 0.125, ((0, 64), (1, 2)))
    value_in = centred(arg_keys[4], (D, RNN), D ** -0.5, 0.125, ((0, 64), (1, 2)))
    pool_mix = centred(arg_keys[5], (GROUPS, GROUP_WIDTH, GROUP_WIDTH), GROUP_WIDTH ** -0.5, 0.5, ((0, 2),))
    averaging_factor = jnp.clip(0.25 + 0.5 * jax.random.uniform(arg_keys[6], (POOL,), jnp.float32) ** shard_levels(arg_keys[6], (POOL,), ((0, 2),), -0.2, 0.2), 0.25, 0.75)
    conv_taps = centred(arg_keys[7], (TAPS, RNN), TAPS ** -0.5, 3.0, ((1, 2),), jnp.float32)
    rate_mix = centred(arg_keys[8], (LOOP_BRANCHES, HEAD_DIM, HEAD_DIM), HEAD_DIM ** -0.5, 0.75, ((0, 2),))
    input_mix = centred(arg_keys[9], (LOOP_BRANCHES, HEAD_DIM, HEAD_DIM), HEAD_DIM ** -0.5, 0.75, ((0, 2),))
    log_rate = draw_log_rate(jax.random.fold_in(arg_keys[15], 71), part)
    decay_shift = draw_decay_shift(jax.random.fold_in(jax.random.fold_in(arg_keys[15], part), 71), part)
    initial_state = centred(part_keys[12], (RNN,), 1.0, 6.0, ((0, 2),), jnp.float32)
    out_pool = centred(arg_keys[13], (D, POOL), (POOL + RNN) ** -0.5, 0.15625, ((0, 64), (1, 2)))
    out_rnn = centred(arg_keys[14], (D, RNN), (POOL + RNN) ** -0.5, 0.15625, ((0, 64), (1, 2)))
    return {"tokens": tokens, "norm_gain": norm_gain, "pool_in": pool_in, "gate_in": gate_in, "value_in": value_in, "pool_mix": pool_mix, "averaging_factor": averaging_factor, "conv_taps": conv_taps, "rate_mix": rate_mix, "input_mix": input_mix, "log_rate": log_rate, "decay_shift": decay_shift, "initial_state": initial_state, "out_pool": out_pool, "out_rnn": out_rnn}


epsilon = 1e-06
sharpness = 8.0

def chain_pairs(first_pair, second_pair):
    return (first_pair[0] * second_pair[0], second_pair[0] * first_pair[1] + second_pair[1])

def reference(tokens, norm_gain, pool_in, gate_in, value_in, pool_mix, averaging_factor, conv_taps, rate_mix, input_mix, log_rate, decay_shift, initial_state, out_pool, out_rnn):
    widened = tokens.astype(jnp.float32)
    scaling = lax.rsqrt(lax.optimization_barrier(jnp.mean(widened * widened, axis=1, keepdims=True)) + epsilon)
    normed = (widened * scaling * norm_gain[None, :]).astype(jnp.bfloat16)
    pool_pre = jnp.dot(normed, pool_in, preferred_element_type=jnp.float32).astype(jnp.bfloat16)
    gate_pre = jnp.dot(normed, gate_in, preferred_element_type=jnp.float32).astype(jnp.bfloat16)
    value_pre = jnp.dot(normed, value_in, preferred_element_type=jnp.float32).astype(jnp.bfloat16)
    pool_values = pool_pre.astype(jnp.float32)
    pool_padded = jnp.pad(pool_values, ((REACH, 0), (0, 0)))
    positions = jnp.arange(TOKEN_COUNT, dtype=jnp.int32)
    pieces = []
    for group_index in range(GROUPS):
        window = 2 ** (group_index + 1)
        low_column = group_index * GROUP_WIDTH
        high_column = low_column + GROUP_WIDTH
        window_sum = jnp.zeros((TOKEN_COUNT, GROUP_WIDTH), jnp.float32)
        for steps_back in range(window):
            window_sum = window_sum + pool_padded[REACH - steps_back:REACH - steps_back + TOKEN_COUNT, low_column:high_column]
        counts = jnp.minimum(positions + 1, window).astype(jnp.float32)[:, None]
        pieces.append(window_sum / counts - pool_values[:, low_column:high_column])
    pooled = jnp.concatenate(pieces, axis=1).astype(jnp.bfloat16)
    mixed_groups = jnp.einsum('tgc,gcd->tgd', pooled.reshape(TOKEN_COUNT, GROUPS, GROUP_WIDTH).astype(jnp.float32), pool_mix.astype(jnp.float32))
    pool_out = (mixed_groups.reshape(TOKEN_COUNT, POOL) * averaging_factor[None, :]).astype(jnp.bfloat16)
    value_padded = jnp.pad(value_pre.astype(jnp.float32), ((TAPS - 1, 0), (0, 0)))
    convolved = conv_taps[0][None, :] * value_padded[0:TOKEN_COUNT]
    for tap_index in range(1, TAPS):
        convolved = convolved + conv_taps[tap_index][None, :] * value_padded[tap_index:tap_index + TOKEN_COUNT]
    conv_out = convolved.astype(jnp.bfloat16)
    conv_heads = conv_out.reshape(TOKEN_COUNT, LOOP_BRANCHES, HEAD_DIM).astype(jnp.float32)
    rate_gate = jax.nn.sigmoid(jnp.einsum('thc,hcd->thd', conv_heads, rate_mix.astype(jnp.float32))).reshape(TOKEN_COUNT, RNN)
    input_gate = jax.nn.sigmoid(jnp.einsum('thc,hcd->thd', conv_heads, input_mix.astype(jnp.float32))).reshape(TOKEN_COUNT, RNN)
    shifts = jnp.broadcast_to(jnp.transpose(decay_shift)[:, :, None], (TOKEN_COUNT, LOOP_BRANCHES, HEAD_DIM)).reshape(TOKEN_COUNT, RNN)
    log_decay = -sharpness * rate_gate * jax.nn.softplus(-log_rate)[None, :] + shifts
    decays = jnp.exp(log_decay)
    drives = jnp.sqrt(-jnp.expm1(2.0 * log_decay)) * input_gate * conv_out.astype(jnp.float32)
    cumulative, local_state = lax.associative_scan(chain_pairs, (decays, drives), axis=0)
    hidden_state = local_state + cumulative * initial_state[None, :]
    rnn_out = (jax.nn.gelu(gate_pre.astype(jnp.float32), approximate=True) * hidden_state).astype(jnp.bfloat16)
    pool_term = jnp.dot(pool_out, jnp.transpose(out_pool), preferred_element_type=jnp.float32)
    rnn_term = jnp.dot(rnn_out, jnp.transpose(out_rnn), preferred_element_type=jnp.float32)
    return (pool_term + rnn_term).astype(jnp.bfloat16)
```

```python
import functools
import math

import jax
import jax.numpy as jnp
from jax import lax
from jax.experimental import pallas as pl
from jax.experimental.pallas import tpu as pltpu
from jax.sharding import PartitionSpec as P

HEAD = 64
LANES = 128
REACH = 16
SEGMENTS = 8
EPSILON = 1e-06
SHARPNESS = 8.0
MESH = pl.DeviceIdType.MESH
F32 = jnp.float32
BF16 = jnp.bfloat16

VALUE = 0
GATES = (512, 896)
POOLS = (768, 1152)
OUT = 1280
PACKED = 2048
WINDOWS = (
    ((0, 256), (512, 384), (1280, 256), (1536, 128)),
    ((256, 256), (896, 384), (1664, 256), (1920, 128)),
)
STARTS = (0, 1, 4, 5)
JOBS = len(STARTS)


def wrapped(index, count):
    return lax.rem(index + count, count)


def log1p_of_exp(v):
    e = jnp.exp(-jnp.abs(v))
    s = e / (2.0 + e)
    q = s * s
    total = jnp.full_like(q, 1.0 / 15.0)
    for odd in (13, 11, 9, 7, 5, 3, 1):
        total = total * q + 1.0 / odd
    return jnp.maximum(v, 0.0) + 2.0 * s * total


def one_minus_exp(y):
    series = jnp.full_like(y, 1.0)
    for k in (9, 8, 7, 6, 5, 4, 3, 2):
        series = 1.0 + series * y * (1.0 / k)
    return jnp.where(y > -0.6, -y * series, 1.0 - jnp.exp(y))


def kernel(ny, nz, *refs):
    (tok_in, gain_in, pool_in, gate_in, value_in, pmix_in, avg_in, taps_in, rmix_in, imix_in,
     lrate_in, shift_in, init_in, opool_in, ornn_in, out,
     w, tok, nrm, proj, aa, bb, acts, shift_t, gain, pmix, avg, taps, rmix, imix, lrate, shift,
     init, bd, soft, ends_a, ends_b, enter, ybuf, zbuf, psend, precv, obuf,
     local_sem, ring_send, ring_recv, pair_send, pair_recv, next_send, next_recv,
     y_send, y_recv, z_send, z_recv, part_send, part_recv, out_sem) = refs
    half, depth = tok_in.shape
    rows = 2 * half
    seg = rows // SEGMENTS
    rnn = lrate.shape[1]
    sp, tp = lax.axis_index("sp"), lax.axis_index("tp")
    z, y = sp // ny, lax.rem(sp, ny)
    count = ny * nz

    def at_y(k):
        return z * ny + wrapped(y + k, ny)

    def at_z(k):
        return wrapped(z + k, nz) * ny + y

    def local(k, src, dst):
        return pltpu.make_async_copy(src, dst, local_sem.at[k])

    mine = w.at[z, y]
    packing = [
        local(0, value_in, mine.at[:, 0:512]),
        local(1, gate_in.at[:, 0:256], mine.at[:, 512:768]),
        local(2, pool_in.at[:, 0:128], mine.at[:, 768:896]),
        local(3, gate_in.at[:, 256:512], mine.at[:, 896:1152]),
        local(4, pool_in.at[:, 128:256], mine.at[:, 1152:1280]),
        local(5, ornn_in, mine.at[:, 1280:1792]),
        local(6, opool_in, mine.at[:, 1792:2048]),
    ]
    my_rows = pl.ds(pl.multiple_of(REACH + tp * half, REACH), half)
    own_tokens = local(7, tok_in, tok.at[my_rows])
    small = [
        local(8 + k, src, dst)
        for k, (src, dst) in enumerate(
            [(gain_in, gain), (pmix_in, pmix), (avg_in, avg), (taps_in, taps), (rmix_in, rmix),
             (imix_in, imix), (lrate_in, lrate), (shift_in, shift), (init_in, init)]
        )
    ]
    for copy in packing + [own_tokens] + small:
        copy.start()

    barrier = pltpu.get_barrier_semaphore()
    peers = [at_y(k) for k in range(1, ny)] + [at_z(k) for k in range(1, nz)]
    peers += [wrapped(sp + 1, count), wrapped(sp - 1, count)]
    for peer in peers:
        pl.semaphore_signal(barrier, inc=1, device_id={"sp": peer}, device_id_type=MESH)
    pl.semaphore_signal(barrier, inc=1, device_id={"tp": 1 - tp}, device_id_type=MESH)
    pl.semaphore_wait(barrier, len(peers) + 1)

    pair = pltpu.make_async_remote_copy(
        src_ref=tok_in, dst_ref=tok.at[my_rows], send_sem=pair_send, recv_sem=pair_recv,
        device_id={"tp": 1 - tp}, device_id_type=MESH,
    )
    pair.start()
    halo = pltpu.make_async_remote_copy(
        src_ref=tok.at[pl.ds(rows, REACH)], dst_ref=tok.at[pl.ds(0, REACH)],
        send_sem=next_send, recv_sem=next_recv,
        device_id={"sp": wrapped(sp + 1, count)}, device_id_type=MESH,
    )

    sizes = ((ny, nz), (nz, ny))
    homes = ((y, z), (z, y))

    def hops(color, job, phase, way):
        n = sizes[color][phase]
        return n // 2 if (way + job + color) % 2 == 0 else (n - 1) // 2

    def block(color, job, phase, origin):
        first, width = WINDOWS[color][job]
        cols = pl.ds(first, width)
        if color == 0:
            return w.at[z, origin, :, cols] if phase == 0 else w.at[origin, :, :, cols]
        return w.at[origin, y, :, cols] if phase == 0 else w.at[:, origin, :, cols]

    def ring(color, job, phase, way, step, arriving):
        n = sizes[color][phase]
        home = homes[color][phase]
        back = step + 1 if arriving else step
        origin = wrapped(home - back if way == 0 else home + back, n)
        on_y = (color == 0) == (phase == 0)
        ahead = 1 if way == 0 else -1
        ref = block(color, job, phase, origin)
        return pltpu.make_async_remote_copy(
            src_ref=ref, dst_ref=ref,
            send_sem=ring_send.at[color, job, phase, way, step],
            recv_sem=ring_recv.at[color, job, phase, way, step],
            device_id={"sp": at_y(ahead) if on_y else at_z(ahead)}, device_id_type=MESH,
        )

    def steps_of(color, job):
        result = []
        for phase in (0, 1):
            for step in range(max(hops(color, job, phase, 0), hops(color, job, phase, 1))):
                result.append([
                    (color, job, phase, way, step) for way in (0, 1)
                    if step < hops(color, job, phase, way)
                ])
        return result

    plans = {(c, j): steps_of(c, j) for c in (0, 1) for j in range(JOBS)}
    started = []

    def advance(color, job, at):
        plan = plans[color, job]
        if 0 < at <= len(plan):
            for key in plan[at - 1]:
                ring(*key, True).wait_recv()
        if 0 <= at < len(plan):
            for key in plan[at]:
                ring(*key, False).start()
                started.append(key)

    def round_of(r):
        if r == 0:
            packing[0].wait()
        if r == STARTS[1]:
            for copy in packing[1:]:
                copy.wait()
        for job in range(JOBS):
            for color in (0, 1):
                advance(color, job, r - STARTS[job])

    def prepare():
        for copy in small:
            copy.wait()
        lane = lax.broadcasted_iota(jnp.int32, (HEAD, LANES), 1)
        for k in range(rnn // LANES):
            for side, mix in enumerate((rmix, imix)):
                both = jnp.concatenate(
                    [mix[2 * k].astype(F32), mix[2 * k + 1].astype(F32)], axis=1
                )
                cols = slice(side * LANES, (side + 1) * LANES)
                bd[k, 0:HEAD, cols] = jnp.where(lane < HEAD, both, 0.0).astype(BF16)
                bd[k, HEAD:LANES, cols] = jnp.where(lane < HEAD, 0.0, both).astype(BF16)
        soft[...] = log1p_of_exp(-lrate[...]) * (-SHARPNESS)
        shift_t[...] = shift[...].T

    def normalize(first, last):
        def body(i, carry):
            at = pl.ds(pl.multiple_of(i * REACH, REACH), REACH)
            x = tok[at, :].astype(F32)
            mean = jnp.sum(x * x, axis=1, keepdims=True) * (1.0 / depth)
            keep = jnp.where(jnp.logical_and(i == 0, sp == 0), 0.0, 1.0)
            nrm[at, :] = (x * lax.rsqrt(mean + EPSILON) * gain[...] * keep).astype(BF16)
            return carry
        lax.fori_loop(first, last, body, 0)

    def project(first, last):
        def body(n, carry):
            cols = pl.ds(pl.multiple_of(n * 256, 256), 256)
            weight = w[:, :, :, cols].reshape(depth, 256)
            result = jnp.dot(nrm[...], weight, preferred_element_type=F32)
            proj[:, cols] = result.astype(BF16).astype(F32)
            return carry
        lax.fori_loop(first, last, body, 0)

    def gates():
        low = lax.broadcasted_iota(jnp.int32, (seg, LANES), 1) < HEAD

        def body(i, carry):
            first = pl.multiple_of(i * seg, seg)
            at = pl.ds(first, seg)
            for k in range(rnn // LANES):
                cols = slice(k * LANES, (k + 1) * LANES)
                v = proj[pl.ds(first, seg + REACH), cols]
                conv = taps[0:1, cols] * v[13:13 + seg]
                for tap in (1, 2, 3):
                    conv = conv + taps[tap:tap + 1, cols] * v[13 + tap:13 + tap + seg]
                conv = conv.astype(BF16)
                terms = jnp.dot(conv, bd[k], preferred_element_type=F32)
                rate = jax.nn.sigmoid(terms[:, :LANES])
                entry = jax.nn.sigmoid(terms[:, LANES:])
                shifts = jnp.where(
                    low, shift_t[at, 2 * k:2 * k + 1], shift_t[at, 2 * k + 1:2 * k + 2]
                )
                log_decay = rate * soft[0:1, cols] + shifts
                aa[k, at, :] = jnp.exp(log_decay)
                bb[k, at, :] = (
                    jnp.sqrt(one_minus_exp(2.0 * log_decay)) * entry * conv.astype(F32)
                )
            return carry
        lax.fori_loop(0, SEGMENTS, body, 0)

    def scan():
        tiles = range(rnn // LANES)

        def body(j, carry):
            at = pl.ds(j, SEGMENTS, stride=seg)
            result = []
            for k in tiles:
                decay, state = carry[k]
                a, b = aa[k, at, :], bb[k, at, :]
                decay = decay * a
                state = a * state + b
                aa[k, at, :] = decay
                bb[k, at, :] = state
                result.append((decay, state))
            return tuple(result)
        start = (jnp.ones((SEGMENTS, LANES), F32), jnp.zeros((SEGMENTS, LANES), F32))
        for k, (decay, state) in enumerate(lax.fori_loop(0, seg, body, (start,) * len(tiles))):
            ends_a[:, k * LANES:(k + 1) * LANES] = decay
            ends_b[:, k * LANES:(k + 1) * LANES] = state
        total_a, total_b = jnp.ones((1, rnn), F32), jnp.zeros((1, rnn), F32)
        for s in range(SEGMENTS):
            enter[s, :, 0:rnn] = total_a
            enter[s, :, rnn:] = total_b
            a, b = ends_a[s:s + 1, :], ends_b[s:s + 1, :]
            total_a, total_b = total_a * a, a * total_b + b
        ybuf[y, :, 0:rnn] = total_a
        ybuf[y, :, rnn:] = total_b

    def to_others(buf, home, n, sends, recvs, target, k, arriving):
        slot = buf.at[wrapped(home - k, n) if arriving else home]
        return pltpu.make_async_remote_copy(
            src_ref=slot, dst_ref=slot, send_sem=sends.at[k], recv_sem=recvs.at[k],
            device_id={"sp": target(k)}, device_id_type=MESH,
        )

    def y_copy(k, arriving):
        return to_others(ybuf, y, ny, y_send, y_recv, at_y, k, arriving)

    def z_copy(k, arriving):
        return to_others(zbuf, z, nz, z_send, z_recv, at_z, k, arriving)

    def chained(buf, n, home):
        whole = before = (jnp.ones((1, rnn), F32), jnp.zeros((1, rnn), F32))
        for s in range(n):
            a, b = buf[s, :, 0:rnn], buf[s, :, rnn:]
            before = tuple(jnp.where(s == home, new, old) for new, old in zip(whole, before))
            whole = (whole[0] * a, a * whole[1] + b)
        return whole, before

    def pool():
        def body(i, carry):
            first = pl.multiple_of(i * seg, seg)
            at = pl.ds(first, seg)
            place = sp * rows + first + lax.broadcasted_iota(jnp.int32, (seg, LANES), 0)
            for g in (0, 1):
                x = proj[pl.ds(first, seg + REACH), POOLS[g]:POOLS[g] + LANES]
                near = x + pltpu.roll(x, 1, 0)
                if g == 1:
                    near = near + pltpu.roll(near, 2, 0)
                far = near
                for width in ((2, 4) if g == 0 else (4, 8)):
                    far = far + pltpu.roll(far, width, 0)
                window = jnp.where(tp == 0, 2 << g, 8 << g)
                summed = jnp.where(tp == 0, near, far)[REACH:]
                counts = jnp.minimum(place + 1, window).astype(F32)
                pooled = (summed / counts - x[REACH:]).astype(BF16)
                mixed = jnp.dot(pooled, pmix[g], preferred_element_type=F32)
                cols = slice(g * LANES, (g + 1) * LANES)
                acts[at, rnn + g * LANES:rnn + (g + 1) * LANES] = (
                    mixed * avg[0:1, cols]
                ).astype(BF16)
            return carry
        lax.fori_loop(0, SEGMENTS, body, 0)

    def gelu():
        scale = math.sqrt(2.0 / math.pi)

        def body(i, carry):
            at = pl.ds(pl.multiple_of(REACH + i * seg, REACH), seg)
            for g in (0, 1):
                cols = slice(GATES[g], GATES[g] + 256)
                x = proj[at, cols]
                proj[at, cols] = x * (
                    0.5 * (1.0 + jnp.tanh(scale * (x + 0.044715 * (x * x * x))))
                )
            return carry
        lax.fori_loop(0, SEGMENTS, body, 0)

    def finish(carried):
        def body(i, carry):
            first = pl.multiple_of(i * seg, seg)
            at = pl.ds(first, seg)
            begin = enter[i, :, 0:rnn] * carried + enter[i, :, rnn:]
            for k in range(rnn // LANES):
                cols = slice(k * LANES, (k + 1) * LANES)
                state = bb[k, at, :] + aa[k, at, :] * begin[:, cols]
                column = GATES[k // 2] + k % 2 * LANES
                gate = proj[pl.ds(pl.multiple_of(REACH + first, REACH), seg),
                            column:column + LANES]
                acts[at, cols] = (gate * state).astype(BF16)
            return carry
        lax.fori_loop(0, SEGMENTS, body, 0)

    features = ny * w.shape[2]

    def part_copy(n):
        return pltpu.make_async_remote_copy(
            src_ref=psend.at[n], dst_ref=precv.at[n], send_sem=part_send.at[n],
            recv_sem=part_recv.at[n], device_id={"tp": 1 - tp}, device_id_type=MESH,
        )

    def product(side, n):
        at = pl.ds(pl.multiple_of(side * half, REACH), half)
        weight = w[n, :, :, OUT:PACKED].reshape(features, PACKED - OUT)
        return lax.dot_general(
            acts[at, :], weight, (((1,), (1,)), ((), ())), preferred_element_type=F32
        )

    def out_copy(n):
        return pltpu.make_async_copy(
            obuf.at[n], out.at[:, pl.ds(pl.multiple_of(n * features, LANES), features)],
            out_sem.at[n],
        )

    round_of(0)
    own_tokens.wait()
    pair.wait_recv()
    halo.start()
    round_of(1)
    prepare()
    round_of(2)
    halo.wait_recv()
    normalize(0, 17)
    round_of(3)
    normalize(17, (rows + REACH) // REACH)
    plan_len = max(len(p) for p in plans.values())
    for r in range(4, plan_len + 1):
        round_of(r)
    project(0, 2)
    round_of(plan_len + 1)
    gates()
    round_of(plan_len + 2)
    scan()
    for k in range(1, ny):
        y_copy(k, False).start()
    round_of(plan_len + 3)
    project(2, 5)
    for k in range(1, ny):
        y_copy(k, True).wait_recv()
    whole, in_row = chained(ybuf, ny, y)
    zbuf[z, :, 0:rnn] = whole[0]
    zbuf[z, :, rnn:] = whole[1]
    for k in range(1, nz):
        z_copy(k, False).start()
    round_of(plan_len + 4)
    pool()
    gelu()
    round_of(plan_len + 5)
    for k in range(1, nz):
        z_copy(k, True).wait_recv()
    _, rows_before = chained(zbuf, nz, z)
    carried = in_row[0] * (rows_before[0] * init[...] + rows_before[1]) + in_row[1]
    finish(carried)

    def to_partner(n, carry):
        psend[n] = product(1 - tp, n).astype(BF16)
        part_copy(n).start()
        return carry

    lax.fori_loop(0, nz, to_partner, 0)

    def for_me(n, carry):
        own = product(tp, n)
        part_copy(n).wait_recv()
        obuf[n] = (own + precv[n].astype(F32)).astype(BF16)
        out_copy(n).start()
        return carry

    lax.fori_loop(0, nz, for_me, 0)

    for key in started:
        ring(*key, False).wait_send()
    pair.wait_send()
    halo.wait_send()
    for k in range(1, ny):
        y_copy(k, False).wait_send()
    for k in range(1, nz):
        z_copy(k, False).wait_send()

    def ended(n, carry):
        part_copy(n).wait_send()
        out_copy(n).wait()
        return carry

    lax.fori_loop(0, nz, ended, 0)


def shards(ny, nz, tokens, norm_gain, pool_in, gate_in, value_in, pool_mix, averaging_factor,
           conv_taps, rate_mix, input_mix, log_rate, decay_shift, initial_state, out_pool,
           out_rnn):
    half, depth = tokens.shape
    rows = 2 * half
    rnn = log_rate.shape[0]
    lines = pool_in.shape[0]
    features = ny * lines
    steps = max(ny, nz) // 2
    dma = pltpu.SemaphoreType.DMA
    vmem = pltpu.VMEM
    scratch = [
        vmem((nz, ny, lines, PACKED), BF16),
        vmem((rows + REACH, depth), BF16),
        vmem((rows + REACH, depth), BF16),
        vmem((rows + REACH, OUT), F32),
        vmem((rnn // LANES, rows, LANES), F32),
        vmem((rnn // LANES, rows, LANES), F32),
        vmem((rows, PACKED - OUT), BF16),
        vmem((rows, rnn // HEAD), F32),
        vmem((1, depth), F32),
        vmem(pool_mix.shape, BF16),
        vmem((1, 2 * LANES), F32),
        vmem(conv_taps.shape, F32),
        vmem(rate_mix.shape, BF16),
        vmem(input_mix.shape, BF16),
        vmem((1, rnn), F32),
        vmem(decay_shift.shape, F32),
        vmem((1, rnn), F32),
        vmem((rnn // LANES, LANES, 2 * LANES), BF16),
        vmem((1, rnn), F32),
        vmem((SEGMENTS, rnn), F32),
        vmem((SEGMENTS, rnn), F32),
        vmem((SEGMENTS, 1, 2 * rnn), F32),
        vmem((ny, 1, 2 * rnn), F32),
        vmem((nz, 1, 2 * rnn), F32),
        vmem((nz, half, features), BF16),
        vmem((nz, half, features), BF16),
        vmem((nz, half, features), BF16),
        dma((17,)),
        dma((2, JOBS, 2, 2, steps)),
        dma((2, JOBS, 2, 2, steps)),
        dma, dma, dma, dma,
        dma((ny,)), dma((ny,)), dma((nz,)), dma((nz,)),
        dma((nz,)), dma((nz,)), dma((nz,)),
    ]
    anywhere = pl.BlockSpec(memory_space=pl.ANY)
    return pl.pallas_call(
        functools.partial(kernel, ny, nz),
        out_shape=jax.ShapeDtypeStruct((half, depth), BF16),
        in_specs=[anywhere] * 15,
        out_specs=anywhere,
        scratch_shapes=scratch,
        compiler_params=pltpu.CompilerParams(
            collective_id=0, has_side_effects=True, vmem_limit_bytes=56 * 1024 * 1024
        ),
        name="layer",
    )(tokens, norm_gain[None], pool_in, gate_in, value_in, pool_mix, averaging_factor[None],
      conv_taps, rate_mix, input_mix, log_rate[None], decay_shift, initial_state[None], out_pool,
      out_rnn)


def grid_of(count):
    ny = 1
    while ny * ny < count:
        ny *= 2
    return ny, count // ny


def solution(mesh):
    ny, nz = grid_of(mesh.shape["sp"])
    placed = (
        P(("fs", "sp", "tp"), None),
        P(),
        P("sp", "tp"),
        P("sp", "tp"),
        P("sp", "tp"),
        P("tp", None, None),
        P("tp"),
        P(None, "tp"),
        P("tp", None, None),
        P("tp", None, None),
        P("tp"),
        P(("fs", "tp"), "sp"),
        P(("fs", "tp")),
        P("sp", "tp"),
        P("sp", "tp"),
    )
    return jax.shard_map(
        functools.partial(shards, ny, nz), mesh=mesh, in_specs=placed,
        out_specs=P(("fs", "sp", "tp"), None), check_vma=False,
    )
```

```python
import functools
import math

import jax
import jax.numpy as jnp
from jax import lax
from jax.experimental import pallas as pl
from jax.experimental.pallas import tpu as pltpu
from jax.sharding import PartitionSpec as P

HEAD = 64
LANES = 128
REACH = 16
SEGMENTS = 8
EPSILON = 1e-06
SHARPNESS = 8.0
MESH = pl.DeviceIdType.MESH
F32 = jnp.float32
BF16 = jnp.bfloat16

GATE = 512
POOL = 1024
OUT = 1280
PACKED = 2048
PITCH = 72
WINDOWS = (
    ("value", 0, 0, 512, 32),
    ("pool", 1, POOL, 256, 16),
    ("gate0", 0, GATE, 256, None),
    ("gate1", 1, GATE + 256, 256, None),
    ("out0", 0, OUT, 256, None),
    ("out1", 1, OUT + 256, 256, None),
    ("out2", 0, OUT + 512, 128, None),
    ("out3", 1, OUT + 640, 128, None),
)
QUARTERS = 4
LINK_RATE = 43e3
HOP = 2.0


def transfers_of(ny, nz, lines):
    table, complete = {}, {}

    def ring(head, axis, n, size, before):
        reached = {0: tuple(before)}
        for way in (1, -1):
            last = tuple(before)
            for step in range(1, n // 2 + 1):
                key = (*head, way, step)
                far = step == n // 2
                table[key] = ((axis, way), size // 2 if far else size, last)
                offset = n // 2 if far else -way * step
                reached[offset] = reached.get(offset, ()) + (key,)
                last = (key,)
        return reached

    def straight(head, axis, n, size):
        reached = {0: ()}
        for step in range(1, n // 2 + 1):
            for way in (1, -1) if step < n // 2 else (1,):
                key = (*head, way, step)
                table[key] = ((axis, way), size * step, ())
                reached[-way * step] = (key,)
        return reached

    for number, (name, order, _, width, rows) in enumerate(WINDOWS):
        (p, np_), (q, nq) = (("y", ny), ("z", nz))[:: -1 if order else 1]
        size = (rows or lines) * (LANES if rows else width) * 2
        first = (straight if rows else ring)(
            (number, 1, 0), p, np_, size, *(() if rows else ((),))
        )
        row = tuple(key for keys in first.values() for key in keys)
        second = ring((number, 2, 0), q, nq, size * np_, row)
        second[0] = row
        keys = set(row).union(*second.values())
        if rows:
            for offset in sorted(second, key=lambda o: (abs(o), o)):
                third = ring((number, 3, offset), "x", QUARTERS, size * np_, second[offset])
                keys = keys.union(*(k for o, k in third.items() if o))
        complete[name] = tuple(k for k in table if k in keys)
    return table, complete


def planned(transfers, tasks):
    clock, free, at, order = 0.0, {}, {}, []
    copies, pieces = dict(transfers), dict(tasks)
    never = 1e9

    def first_ready(table):
        for key, entry in table.items():
            if all(at.get(other, never) <= clock for other in entry[-1]):
                return key
        return None

    while copies or pieces:
        key = first_ready(copies)
        if key is not None:
            link, size, _ = copies.pop(key)
            begin = max(clock, free.get(link, 0.0))
            free[link] = begin + size / LINK_RATE
            at[key] = free[link] + HOP
            clock += 0.02
            order.append(key)
            continue
        key = first_ready(pieces)
        if key is not None:
            cost, _ = pieces.pop(key)
            clock += cost
            at[key] = clock
            order.append(key)
            continue
        clock = min(time for time in at.values() if time > clock)
    return order


def wrapped(index, count):
    return lax.rem(index + count, count)


def log1p_of_exp(v):
    e = jnp.exp(-jnp.abs(v))
    s = e / (2.0 + e)
    q = s * s
    total = jnp.full_like(q, 1.0 / 15.0)
    for odd in (13, 11, 9, 7, 5, 3, 1):
        total = total * q + 1.0 / odd
    return jnp.maximum(v, 0.0) + 2.0 * s * total


def one_minus_exp(y):
    series = jnp.full_like(y, 1.0)
    for k in (9, 8, 7, 6, 5, 4, 3, 2):
        series = 1.0 + series * y * (1.0 / k)
    return jnp.where(y > -0.6, -y * series, 1.0 - jnp.exp(y))


def kernel(ny, nz, *refs):
    (tok_in, gain_in, pool_in, gate_in, value_in, pmix_in, avg_in, taps_in, rmix_in, imix_in,
     lrate_in, shift_in, init_in, opool_in, ornn_in, out,
     w, tok, nrm, proj, aa, bb, acts, shift_t, gain, pmix, avg, taps, rmix, imix, lrate, shift,
     init, bd, soft, ends_a, ends_b, enter, carried, ybuf, zbuf, psend, precv, own, obuf,
     local_sem, ring_send, ring_recv, pair_send, pair_recv, next_send, next_recv,
     y_send, y_recv, z_send, z_recv, part_send, part_recv, out_sem) = refs
    half, depth = tok_in.shape
    rows = 2 * half
    seg = rows // SEGMENTS
    rnn = lrate.shape[1]
    sp, tp = lax.axis_index("sp"), lax.axis_index("tp")
    z, y, x = sp // ny, lax.rem(sp, ny), lax.axis_index("fs")
    count = ny * nz

    def at_y(k):
        return z * ny + wrapped(y + k, ny)

    def at_z(k):
        return wrapped(z + k, nz) * ny + y

    def local(k, src, dst):
        return pltpu.make_async_copy(src, dst, local_sem.at[k])

    mine = w.at[z, y]
    lane = pl.multiple_of(x * LANES, LANES)
    pool_lane = pl.multiple_of(x // 2 * LANES, LANES)
    pool_lines = pl.ds(pl.multiple_of(lax.rem(x, 2) * 16, 16), 16)
    packing = [
        local(0, value_in.at[:, pl.ds(lane, LANES)], mine.at[:, pl.ds(lane, LANES)]),
        local(1, pool_in.at[pool_lines, pl.ds(pool_lane, LANES)],
              mine.at[pool_lines, pl.ds(POOL + pool_lane, LANES)]),
        local(2, gate_in, mine.at[:, GATE:POOL]),
        local(3, ornn_in, mine.at[:, OUT:OUT + rnn]),
        local(4, opool_in, mine.at[:, OUT + rnn:PACKED]),
    ]
    my_rows = pl.ds(pl.multiple_of(REACH + tp * half, REACH), half)
    own_tokens = local(5, tok_in, tok.at[my_rows])
    small = [
        local(6 + k, src, dst)
        for k, (src, dst) in enumerate(
            [(gain_in, gain), (pmix_in, pmix), (avg_in, avg), (taps_in, taps), (rmix_in, rmix),
             (imix_in, imix), (lrate_in, lrate), (shift_in, shift), (init_in, init)]
        )
    ]
    for copy in packing + [own_tokens] + small:
        copy.start()

    barrier = pltpu.get_barrier_semaphore()
    peers = [at_y(k) for k in range(1, ny)] + [at_z(k) for k in range(1, nz)]
    peers += [wrapped(sp + 1, count), wrapped(sp - 1, count)]
    for peer in peers:
        pl.semaphore_signal(barrier, inc=1, device_id={"sp": peer}, device_id_type=MESH)
    pl.semaphore_signal(barrier, inc=1, device_id={"tp": 1 - tp}, device_id_type=MESH)
    for way in (1, -1):
        pl.semaphore_signal(
            barrier, inc=1, device_id={"fs": wrapped(x + way, QUARTERS)}, device_id_type=MESH
        )
    for copy in packing:
        copy.wait()
    pl.semaphore_wait(barrier, len(peers) + 3)

    pair = pltpu.make_async_remote_copy(
        src_ref=tok_in, dst_ref=tok.at[my_rows], send_sem=pair_send, recv_sem=pair_recv,
        device_id={"tp": 1 - tp}, device_id_type=MESH,
    )
    halo = pltpu.make_async_remote_copy(
        src_ref=tok.at[pl.ds(rows, REACH)], dst_ref=tok.at[pl.ds(0, REACH)],
        send_sem=next_send, recv_sem=next_recv,
        device_id={"sp": wrapped(sp + 1, count)}, device_id_type=MESH,
    )

    table, complete = transfers_of(ny, nz, w.shape[2])
    places = {key: k for k, key in enumerate(table)}
    groups = {}
    for key in table:
        groups.setdefault(key[:3], len(groups))
    sizes = {"y": ny, "z": nz, "x": QUARTERS}
    homes = {"y": y, "z": z, "x": x}

    def region(number, phase, offset, origin, half):
        _, order, first, width, rows = WINDOWS[number]
        p, q = ("z", "y") if order else ("y", "z")
        at = {p: slice(None), q: homes[q]}
        if phase == 1:
            at[p] = wrapped(homes[p] + origin, sizes[p])
        else:
            at[q] = wrapped(homes[q] + (origin if phase == 2 else offset), sizes[q])
            if half is not None:
                at[p] = pl.ds(half * (sizes[p] // 2), sizes[p] // 2)
        lines, cols = slice(None), pl.ds(first, width)
        if rows:
            part = wrapped(x + origin, QUARTERS) if phase == 3 else x
            if rows < w.shape[2]:
                lines = pl.ds(pl.multiple_of(lax.rem(part, 2) * rows, rows), rows)
                part = part // 2
            cols = pl.ds(pl.multiple_of(first + part * LANES, LANES), LANES)
        elif phase == 1 and half is not None:
            lines = pl.ds(half * 16, 16)
        return w.at[at["z"], at["y"], lines, cols]

    def gather_copy(key, arriving):
        number, phase, offset, way, step = key
        _, order, _, _, rows = WINDOWS[number]
        straight = rows and phase == 1
        axis = table[key][0][0]
        far = step == sizes[axis] // 2 and not straight
        origin = -way * (step if arriving else 0 if straight else step - 1)
        ref = region(number, phase, offset, origin, (1 - way) // 2 if far else None)
        ahead = way * (step if straight else 1)
        target = {
            "y": lambda: {"sp": at_y(ahead)},
            "z": lambda: {"sp": at_z(ahead)},
            "x": lambda: {"fs": wrapped(x + ahead, QUARTERS)},
        }[axis]()
        return pltpu.make_async_remote_copy(
            src_ref=ref, dst_ref=ref, send_sem=ring_send.at[groups[key[:3]]],
            recv_sem=ring_recv.at[places[key]], device_id=target, device_id_type=MESH,
        )

    def all_sent(group):
        number, phase, _ = group
        _, order, first, width, rows = WINDOWS[number]
        lines = slice(0, rows or w.shape[2])
        cols = slice(first, first + (LANES if rows else width))
        if phase == 3:
            cols = slice(0, (QUARTERS - 1) * LANES)
            ref = w.at[:, 0, lines, cols] if order else w.at[0, :, lines, cols]
        elif (phase == 1) == (order == 0):
            lead = slice(0, ny - 1)
            ref = w.at[0 if phase == 1 else slice(None), lead, lines, cols]
        else:
            lead = slice(0, nz - 1)
            ref = w.at[lead, 0 if phase == 1 else slice(None), lines, cols]
        sem = ring_send.at[groups[group]]
        pltpu.make_async_copy(ref, ref, sem).wait()

    def prepare():
        for copy in small:
            copy.wait()
        lane = lax.broadcasted_iota(jnp.int32, (HEAD, LANES), 1)
        for k in range(rnn // LANES):
            for side, mix in enumerate((rmix, imix)):
                both = jnp.concatenate(
                    [mix[2 * k].astype(F32), mix[2 * k + 1].astype(F32)], axis=1
                )
                cols = slice(side * LANES, (side + 1) * LANES)
                bd[k, 0:HEAD, cols] = jnp.where(lane < HEAD, both, 0.0).astype(BF16)
                bd[k, HEAD:LANES, cols] = jnp.where(lane < HEAD, 0.0, both).astype(BF16)
        soft[...] = log1p_of_exp(-lrate[...]) * (-SHARPNESS)
        shift_t[...] = shift[...].T

    def normalize(first, last):
        def body(i, carry):
            at = pl.ds(pl.multiple_of(i * REACH, REACH), REACH)
            x = tok[at, :].astype(F32)
            mean = jnp.sum(x * x, axis=1, keepdims=True) * (1.0 / depth)
            keep = jnp.where(jnp.logical_and(i == 0, sp == 0), 0.0, 1.0)
            nrm[at, :] = (x * lax.rsqrt(mean + EPSILON) * gain[...] * keep).astype(BF16)
            return carry
        lax.fori_loop(first, last, body, 0, unroll=3)

    def project(first, last):
        def body(n, carry):
            cols = pl.ds(pl.multiple_of(n * 256, 256), 256)
            weight = w[:, :, :, cols].reshape(depth, 256)
            result = jnp.dot(nrm[...], weight, preferred_element_type=F32)
            proj[:, cols] = result.astype(BF16).astype(F32)
            return carry
        lax.fori_loop(first, last, body, 0)

    def gates(begin, end):
        low = lax.broadcasted_iota(jnp.int32, (seg, LANES), 1) < HEAD

        def body(i, carry):
            first = pl.multiple_of(i * seg, seg)
            at = pl.ds(first, seg)
            for k in range(rnn // LANES):
                cols = slice(k * LANES, (k + 1) * LANES)
                v = proj[pl.ds(first, seg + REACH), cols]
                conv = taps[0:1, cols] * v[13:13 + seg]
                for tap in (1, 2, 3):
                    conv = conv + taps[tap:tap + 1, cols] * v[13 + tap:13 + tap + seg]
                conv = conv.astype(BF16)
                terms = jnp.dot(conv, bd[k], preferred_element_type=F32)
                rate = jax.nn.sigmoid(terms[:, :LANES])
                entry = jax.nn.sigmoid(terms[:, LANES:])
                shifts = jnp.where(
                    low, shift_t[at, 2 * k:2 * k + 1], shift_t[at, 2 * k + 1:2 * k + 2]
                )
                log_decay = rate * soft[0:1, cols] + shifts
                put = pl.ds(pl.multiple_of(i * PITCH, 8), seg)
                aa[k, put, :] = jnp.exp(log_decay)
                bb[k, put, :] = (
                    jnp.sqrt(one_minus_exp(2.0 * log_decay)) * entry * conv.astype(F32)
                )
            return carry
        lax.fori_loop(begin, end, body, 0)

    def scan():
        tiles = range(rnn // LANES)

        def body(j, carry):
            at = pl.ds(j, SEGMENTS, stride=PITCH)
            result = []
            for k in tiles:
                decay, state = carry[k]
                a, b = aa[k, at, :], bb[k, at, :]
                decay = decay * a
                state = a * state + b
                aa[k, at, :] = decay
                bb[k, at, :] = state
                result.append((decay, state))
            return tuple(result)
        start = (jnp.ones((SEGMENTS, LANES), F32), jnp.zeros((SEGMENTS, LANES), F32))
        for k, (decay, state) in enumerate(lax.fori_loop(0, seg, body, (start,) * len(tiles))):
            ends_a[:, k * LANES:(k + 1) * LANES] = decay
            ends_b[:, k * LANES:(k + 1) * LANES] = state
        total_a, total_b = jnp.ones((1, rnn), F32), jnp.zeros((1, rnn), F32)
        for s in range(SEGMENTS):
            enter[s, :, 0:rnn] = total_a
            enter[s, :, rnn:] = total_b
            a, b = ends_a[s:s + 1, :], ends_b[s:s + 1, :]
            total_a, total_b = total_a * a, a * total_b + b
        ybuf[y, :, 0:rnn] = total_a
        ybuf[y, :, rnn:] = total_b

    def to_others(buf, home, n, sends, recvs, target, k, arriving):
        slot = buf.at[wrapped(home - k, n) if arriving else home]
        return pltpu.make_async_remote_copy(
            src_ref=slot, dst_ref=slot, send_sem=sends.at[k], recv_sem=recvs.at[k],
            device_id={"sp": target(k)}, device_id_type=MESH,
        )

    def y_copy(k, arriving):
        return to_others(ybuf, y, ny, y_send, y_recv, at_y, k, arriving)

    def z_copy(k, arriving):
        return to_others(zbuf, z, nz, z_send, z_recv, at_z, k, arriving)

    def chained(buf, n, home):
        whole = before = (jnp.ones((1, rnn), F32), jnp.zeros((1, rnn), F32))
        for s in range(n):
            a, b = buf[s, :, 0:rnn], buf[s, :, rnn:]
            before = tuple(jnp.where(s == home, new, old) for new, old in zip(whole, before))
            whole = (whole[0] * a, a * whole[1] + b)
        return whole, before

    def turned(first):
        return pl.ds(pl.multiple_of(lax.rem(first + (1 - tp) * half, rows), REACH), seg)

    def pool():
        def body(i, carry):
            first = pl.multiple_of(i * seg, seg)
            at = turned(first)
            place = sp * rows + first + lax.broadcasted_iota(jnp.int32, (seg, LANES), 0)
            for g in (0, 1):
                x = proj[pl.ds(first, seg + REACH), POOL + g * LANES:POOL + (g + 1) * LANES]
                near = x + pltpu.roll(x, 1, 0)
                if g == 1:
                    near = near + pltpu.roll(near, 2, 0)
                far = near
                for width in ((2, 4) if g == 0 else (4, 8)):
                    far = far + pltpu.roll(far, width, 0)
                window = jnp.where(tp == 0, 2 << g, 8 << g)
                summed = jnp.where(tp == 0, near, far)[REACH:]
                counts = jnp.minimum(place + 1, window).astype(F32)
                pooled = (summed / counts - x[REACH:]).astype(BF16)
                mixed = jnp.dot(pooled, pmix[g], preferred_element_type=F32)
                cols = slice(g * LANES, (g + 1) * LANES)
                acts[at, rnn + g * LANES:rnn + (g + 1) * LANES] = (
                    mixed * avg[0:1, cols]
                ).astype(BF16)
            return carry
        lax.fori_loop(0, SEGMENTS, body, 0)

    def gelu():
        scale = math.sqrt(2.0 / math.pi)

        def body(i, carry):
            at = pl.ds(pl.multiple_of(REACH + i * seg, REACH), seg)
            cols = slice(GATE, POOL)
            v = proj[at, cols]
            proj[at, cols] = v * (0.5 * (1.0 + jnp.tanh(scale * (v + 0.044715 * (v * v * v)))))
            return carry
        lax.fori_loop(0, SEGMENTS, body, 0)

    def carry_in():
        _, rows_before = chained(zbuf, nz, z)
        _, in_row = chained(ybuf, ny, y)
        entry = rows_before[0] * init[...] + rows_before[1]
        carried[...] = in_row[0] * entry + in_row[1]

    def row_total():
        whole, _ = chained(ybuf, ny, y)
        zbuf[z, :, 0:rnn] = whole[0]
        zbuf[z, :, rnn:] = whole[1]

    def finish():
        def body(i, carry):
            first = pl.multiple_of(i * seg, seg)
            at = pl.ds(pl.multiple_of(i * PITCH, 8), seg)
            put = turned(first)
            begin = enter[i, :, 0:rnn] * carried[...] + enter[i, :, rnn:]
            for k in range(rnn // LANES):
                cols = slice(k * LANES, (k + 1) * LANES)
                state = bb[k, at, :] + aa[k, at, :] * begin[:, cols]
                gate = proj[pl.ds(pl.multiple_of(REACH + first, REACH), seg),
                            GATE + k * LANES:GATE + (k + 1) * LANES]
                acts[put, cols] = (gate * state).astype(BF16)
            return carry
        lax.fori_loop(0, SEGMENTS, body, 0)

    features = ny * w.shape[2]

    def part_copy(n):
        return pltpu.make_async_remote_copy(
            src_ref=psend.at[n], dst_ref=precv.at[n], send_sem=part_send.at[n],
            recv_sem=part_recv.at[n], device_id={"tp": 1 - tp}, device_id_type=MESH,
        )

    def products():
        def body(n, carry):
            weight = w[n, :, :, OUT:PACKED].reshape(features, PACKED - OUT)
            result = lax.dot_general(
                acts[...], weight, (((1,), (1,)), ((), ())), preferred_element_type=F32
            )
            psend[n] = result[:half].astype(BF16)
            part_copy(n).start()
            own[n] = result[half:]
            return carry
        lax.fori_loop(0, nz, body, 0)

    def out_copy(n):
        return pltpu.make_async_copy(
            obuf.at[n], out.at[:, pl.ds(pl.multiple_of(n * features, LANES), features)],
            out_sem.at[n],
        )

    def totals():
        def body(n, carry):
            part_copy(n).wait_recv()
            obuf[n] = (own[n] + precv[n].astype(F32)).astype(BF16)
            out_copy(n).start()
            return carry
        lax.fori_loop(0, nz, body, 0)

    copies = {"pair": (None, 0, ()), "halo": (None, 0, ("pair", "own"))}
    copies.update({"y_sums": (None, 0, ("scan",)), "z_sums": (None, 0, ("row_total",))})
    copies.update(table)
    blocks = (rows + REACH) // REACH
    cuts = [blocks * k // 4 // 3 * 3 for k in range(4)] + [blocks]
    normed = tuple(f"norm{k}" for k in range(4))
    pieces = {"own": (0.0, own_tokens.wait, ()), "prepare": (0.3, prepare, ())}
    for k in range(4):
        pieces[normed[k]] = (
            0.8, functools.partial(normalize, cuts[k], cuts[k + 1]), ("halo",)
        )
    for k in range(2):
        pieces[f"value{k}"] = (
            0.8, functools.partial(project, k, k + 1), complete["value"] + normed
        )
    for k in range(4):
        pieces[f"gates{k}"] = (
            0.8, functools.partial(gates, 2 * k, 2 * k + 2), ("value0", "value1", "prepare")
        )
    pieces["scan"] = (1.5, scan, tuple(f"gates{k}" for k in range(4)))
    pieces["row_total"] = (0.1, row_total, ("y_sums",))
    pieces["carry_in"] = (0.1, carry_in, ("z_sums",))
    for k in range(2):
        pieces[f"gate{k}"] = (
            0.8, functools.partial(project, 2 + k, 3 + k), complete[f"gate{k}"] + normed
        )
    pieces["project_pool"] = (0.8, functools.partial(project, 4, 5), complete["pool"] + normed)
    pieces["gelu"] = (0.4, gelu, ("gate0", "gate1"))
    pieces["pool"] = (1.4, pool, ("project_pool", "prepare"))
    pieces["finish"] = (0.3, finish, ("carry_in", "gelu"))
    outs = sum((complete[f"out{k}"] for k in range(4)), ())
    pieces["products"] = (2.5, products, ("finish", "pool") + outs)
    pieces["totals"] = (1.5, totals, ("products",))

    def y_all(arriving):
        return [y_copy(k, arriving) for k in range(1, ny)]

    def z_all(arriving):
        return [z_copy(k, arriving) for k in range(1, nz)]

    def started(key, arriving):
        if key == "pair":
            return [pair]
        if key == "halo":
            return [halo]
        if key == "y_sums":
            return y_all(arriving)
        if key == "z_sums":
            return z_all(arriving)
        return [gather_copy(key, arriving)]

    waited = set()

    def settle(keys):
        for key in keys:
            if key in copies and key not in waited:
                waited.add(key)
                for copy in started(key, True):
                    copy.wait_recv()

    for key in planned(copies, {k: (v[0], v[2]) for k, v in pieces.items()}):
        if key in copies:
            settle(copies[key][-1])
            for copy in started(key, False):
                copy.start()
        else:
            settle(pieces[key][-1])
            pieces[key][1]()
    settle(copies)

    for group in groups:
        all_sent(group)
    for key in ("pair", "halo", "y_sums", "z_sums"):
        for copy in started(key, False):
            copy.wait_send()

    def ended(n, carry):
        part_copy(n).wait_send()
        out_copy(n).wait()
        return carry

    lax.fori_loop(0, nz, ended, 0)


def shards(ny, nz, tokens, norm_gain, pool_in, gate_in, value_in, pool_mix, averaging_factor,
           conv_taps, rate_mix, input_mix, log_rate, decay_shift, initial_state, out_pool,
           out_rnn):
    half, depth = tokens.shape
    rows = 2 * half
    rnn = log_rate.shape[0]
    lines = pool_in.shape[0]
    features = ny * lines
    table, _ = transfers_of(ny, nz, lines)
    dma = pltpu.SemaphoreType.DMA
    vmem = pltpu.VMEM
    scratch = [
        vmem((nz, ny, lines, PACKED), BF16),
        vmem((rows + REACH, depth), BF16),
        vmem((rows + REACH, depth), BF16),
        vmem((rows + REACH, OUT), F32),
        vmem((rnn // LANES, SEGMENTS * PITCH, LANES), F32),
        vmem((rnn // LANES, SEGMENTS * PITCH, LANES), F32),
        vmem((rows, PACKED - OUT), BF16),
        vmem((rows, rnn // HEAD), F32),
        vmem((1, depth), F32),
        vmem(pool_mix.shape, BF16),
        vmem((1, 2 * LANES), F32),
        vmem(conv_taps.shape, F32),
        vmem(rate_mix.shape, BF16),
        vmem(input_mix.shape, BF16),
        vmem((1, rnn), F32),
        vmem(decay_shift.shape, F32),
        vmem((1, rnn), F32),
        vmem((rnn // LANES, LANES, 2 * LANES), BF16),
        vmem((1, rnn), F32),
        vmem((SEGMENTS, rnn), F32),
        vmem((SEGMENTS, rnn), F32),
        vmem((SEGMENTS, 1, 2 * rnn), F32),
        vmem((1, rnn), F32),
        vmem((ny, 1, 2 * rnn), F32),
        vmem((nz, 1, 2 * rnn), F32),
        vmem((nz, half, features), BF16),
        vmem((nz, half, features), BF16),
        vmem((nz, half, features), F32),
        vmem((nz, half, features), BF16),
        dma((15,)),
        dma((len({key[:3] for key in table}),)),
        dma((len(table),)),
        dma, dma, dma, dma,
        dma((ny,)), dma((ny,)), dma((nz,)), dma((nz,)),
        dma((nz,)), dma((nz,)), dma((nz,)),
    ]
    anywhere = pl.BlockSpec(memory_space=pl.ANY)
    return pl.pallas_call(
        functools.partial(kernel, ny, nz),
        out_shape=jax.ShapeDtypeStruct((half, depth), BF16),
        in_specs=[anywhere] * 15,
        out_specs=anywhere,
        scratch_shapes=scratch,
        compiler_params=pltpu.CompilerParams(
            collective_id=0, has_side_effects=True, vmem_limit_bytes=56 * 1024 * 1024
        ),
        name="layer",
    )(tokens, norm_gain[None], pool_in, gate_in, value_in, pool_mix, averaging_factor[None],
      conv_taps, rate_mix, input_mix, log_rate[None], decay_shift, initial_state[None], out_pool,
      out_rnn)


def grid_of(count):
    ny = 1
    while ny * ny < count:
        ny *= 2
    return ny, count // ny


def solution(mesh):
    ny, nz = grid_of(mesh.shape["sp"])
    placed = (
        P(("fs", "sp", "tp"), None),
        P(),
        P("sp", "tp"),
        P("sp", "tp"),
        P("sp", "tp"),
        P("tp", None, None),
        P("tp"),
        P(None, "tp"),
        P("tp", None, None),
        P("tp", None, None),
        P("tp"),
        P(("fs", "tp"), "sp"),
        P(("fs", "tp")),
        P("sp", "tp"),
        P("sp", "tp"),
    )
    return jax.shard_map(
        functools.partial(shards, ny, nz), mesh=mesh, in_specs=placed,
        out_specs=P(("fs", "sp", "tp"), None), check_vma=False,
    )
```

```python
import functools
import math

import jax
import jax.numpy as jnp
from jax import lax
from jax.experimental import pallas as pl
from jax.experimental.pallas import tpu as pltpu
from jax.sharding import PartitionSpec as P

HEAD = 64
LANES = 128
REACH = 16
SEGMENTS = 8
EPSILON = 1e-06
SHARPNESS = 8.0
MESH = pl.DeviceIdType.MESH
F32 = jnp.float32
BF16 = jnp.bfloat16

VALUE = 0
GATE = 512
POOL = 1024
OUT = 1280
PACKED = 2048
PITCH = 72
WINDOWS = (
    ("value", 0, 0, 256, True, None),
    ("gate", 0, GATE, 256, True, 1),
    ("gate", 1, GATE + 384, 128, False, None),
    ("gate", 0, GATE + 256, 128, False, 1),
    ("value", 1, 256, 256, True, None),
    ("pool", 1, POOL, 256, True, 2),
    ("out", 0, OUT, 128, False, 3),
    ("out", 0, OUT + 128, 256, False, 2),
    ("out", 1, OUT + 384, 256, False, 3),
    ("out", 1, OUT + 640, 128, False, None),
)
X_RING = 4
LINK_RATE = 40e3
HOP = 2.2


def transfers_of(ny, nz, lines):
    table, complete = {}, {}

    def ring(head, axis, n, size, before):
        reached = {0: tuple(before)}
        for way in (1, -1):
            last = tuple(before)
            for step in range(1, n // 2 + 1):
                key = (*head, way, step)
                far = step == n // 2
                table[key] = ((axis, way), size // 2 if far else size, last)
                offset = n // 2 if far else -way * step
                reached[offset] = reached.get(offset, ()) + (key,)
                last = (key,)
        return reached

    def straight(head, axis, n, size):
        reached = {0: ()}
        for step in range(1, n // 2 + 1):
            for way in (1, -1) if step < n // 2 else (1,):
                key = (*head, way, step)
                table[key] = ((axis, way), size * step, ())
                reached[-way * step] = (key,)
        return reached

    for number, (name, order, _, width, shared, hold) in enumerate(WINDOWS):
        (p, np_), (q, nq) = (("y", ny), ("z", nz))[:: -1 if order else 1]
        size = lines * (width // 2 if shared else width) * 2
        first = straight((number, 1, 0), p, np_, size) if shared else ring(
            (number, 1, 0), p, np_, size, ()
        )
        row = tuple(key for keys in first.values() for key in keys)
        second = ring((number, 2, 0), q, nq, size * np_, row)
        second[0] = row
        if hold is not None:
            leader = [w[:2] for w in WINDOWS].index(("value", order))
            for way in (1, -1):
                link, size_, before = table[number, 2, 0, way, 1]
                sent = ("sent", (leader, 2, 0, way, min(hold, nq // 2)))
                table[number, 2, 0, way, 1] = (link, size_, before + (sent,))
        keys = set(row).union(*second.values())
        if shared:
            for offset in sorted(second, key=lambda o: (abs(o), o)):
                for way in (1, -1):
                    key = (number, 3, offset, way, 1)
                    table[key] = (("x", way), size * np_ // 2, second[offset])
                    keys.add(key)
        complete[name] = complete.get(name, ()) + tuple(k for k in table if k in keys)
    return table, complete


def semaphores_of(table, ny, nz):
    sends, recvs = {}, {}
    for key in table:
        number, phase, _, _, step = key
        order, shared = WINDOWS[number][1], WINDOWS[number][4]
        n = (ny, nz)[(phase - 1) ^ order] if phase < 3 else 0
        together = phase == 3 or (shared and phase == 1) or step == n // 2
        recvs[key] = (number, phase, "all" if phase == 3 or (shared and phase == 1) else "far") \
            if together else key
        sends[key] = (number, phase)
    return sends, recvs


def planned(transfers, tasks):
    clock, free, at, order = 0.0, {}, {}, []
    copies, pieces = dict(transfers), dict(tasks)
    never = 1e9

    def first_ready(table):
        for key, entry in table.items():
            if all(at.get(other, never) <= clock for other in entry[-1]):
                return key
        return None

    while copies or pieces:
        key = first_ready(copies)
        if key is not None:
            link, size, _ = copies.pop(key)
            begin = max(clock, free.get(link, 0.0)) if link else clock
            free[link] = begin + size / LINK_RATE
            at[key] = free[link] + HOP * (1 if link else 2)
            at["sent", key] = clock
            clock += 0.02
            order.append(key)
            continue
        key = first_ready(pieces)
        if key is not None:
            cost, _ = pieces.pop(key)
            clock += cost
            at[key] = clock
            order.append(key)
            continue
        clock = min(time for time in at.values() if time > clock)
    return order


def wrapped(index, count):
    return lax.rem(index + count, count)


def log1p_of_exp(v):
    e = jnp.exp(-jnp.abs(v))
    s = e / (2.0 + e)
    q = s * s
    total = jnp.full_like(q, 1.0 / 15.0)
    for odd in (13, 11, 9, 7, 5, 3, 1):
        total = total * q + 1.0 / odd
    return jnp.maximum(v, 0.0) + 2.0 * s * total


def one_minus_square(a, x):
    v = 2.0 * x
    series = jnp.full_like(v, 1.0 / 720.0)
    for k in (120.0, 24.0, 6.0, 2.0, 1.0):
        series = series * v + 1.0 / k
    return jnp.where(v > -0.25, -v * series, 1.0 - a * a)


def kernel(ny, nz, *refs):
    (tok_in, gain_in, pool_in, gate_in, value_in, pmix_in, avg_in, taps_in, rmix_in, imix_in,
     lrate_in, shift_in, init_in, opool_in, ornn_in, out,
     w, tok, nrm, proj, aa, bb, acts, shift_t, gain, pmix, avg, taps, rmix, imix, lrate, shift,
     init, bd, soft, ends_a, ends_b, enter, carried, ybuf, zbuf, psend, precv, own, obuf,
     local_sem, ring_send, ring_recv, pair_send, pair_recv, next_send, next_recv,
     y_sem, z_sem, part_send, part_recv, out_sem) = refs
    half, depth = tok_in.shape
    rows = 2 * half
    seg = rows // SEGMENTS
    rnn = lrate.shape[1]
    sp, tp = lax.axis_index("sp"), lax.axis_index("tp")
    z, y, x = sp // ny, lax.rem(sp, ny), lax.axis_index("fs")
    count = ny * nz

    def at_y(k):
        return z * ny + wrapped(y + k, ny)

    def at_z(k):
        return wrapped(z + k, nz) * ny + y

    def local(k, src, dst):
        return pltpu.make_async_copy(src, dst, local_sem.at[k])

    mine = w.at[z, y]
    parity = lax.rem(x, 2)
    sources = {"value": (value_in, 0), "gate": (gate_in, GATE), "pool": (pool_in, POOL)}
    packing = []
    for name, _, first, width, shared, _ in WINDOWS:
        if name in sources:
            src, base = sources[name]
            if shared:
                skip, width = pl.multiple_of(parity * LANES, LANES), width // 2
                cols, from_ = pl.ds(first + skip, width), pl.ds(first - base + skip, width)
            else:
                cols, from_ = pl.ds(first, width), pl.ds(first - base, width)
            packing.append(local(len(packing), src.at[:, from_], mine.at[:, cols]))
    packing.append(local(len(packing), ornn_in, mine.at[:, OUT:OUT + rnn]))
    packing.append(local(len(packing), opool_in, mine.at[:, OUT + rnn:PACKED]))
    my_rows = pl.ds(pl.multiple_of(REACH + tp * half, REACH), half)
    own_tokens = local(8, tok_in, tok.at[my_rows])
    small = [
        local(9 + k, src, dst)
        for k, (src, dst) in enumerate(
            [(gain_in, gain), (pmix_in, pmix), (avg_in, avg), (taps_in, taps), (rmix_in, rmix),
             (imix_in, imix), (lrate_in, lrate), (shift_in, shift), (init_in, init)]
        )
    ]
    for copy in packing + [own_tokens] + small:
        copy.start()

    barrier = pltpu.get_barrier_semaphore()
    peers = [at_y(k) for k in range(1, ny)] + [at_z(k) for k in range(1, nz)]
    peers += [wrapped(sp + 1, count), wrapped(sp - 1, count)]
    for peer in peers:
        pl.semaphore_signal(barrier, inc=1, device_id={"sp": peer}, device_id_type=MESH)
    pl.semaphore_signal(barrier, inc=1, device_id={"tp": 1 - tp}, device_id_type=MESH)
    for way in (1, -1):
        pl.semaphore_signal(
            barrier, inc=1, device_id={"fs": wrapped(x + way, X_RING)}, device_id_type=MESH
        )
    for copy in packing:
        copy.wait()
    pl.semaphore_wait(barrier, len(peers) + 3)

    pair = pltpu.make_async_remote_copy(
        src_ref=tok_in, dst_ref=tok.at[my_rows], send_sem=pair_send, recv_sem=pair_recv,
        device_id={"tp": 1 - tp}, device_id_type=MESH,
    )
    halo = pltpu.make_async_remote_copy(
        src_ref=tok.at[pl.ds(rows, REACH)], dst_ref=tok.at[pl.ds(0, REACH)],
        send_sem=next_send, recv_sem=next_recv,
        device_id={"sp": wrapped(sp + 1, count)}, device_id_type=MESH,
    )

    table, complete = transfers_of(ny, nz, w.shape[2])
    sends, recvs = semaphores_of(table, ny, nz)
    send_at = {group: k for k, group in enumerate(dict.fromkeys(sends.values()))}
    recv_at = {group: k for k, group in enumerate(dict.fromkeys(recvs.values()))}
    sizes = {"y": ny, "z": nz}
    homes = {"y": y, "z": z}

    def region(key, arriving):
        number, phase, offset, way, step = key
        _, order, first, width, shared, _ = WINDOWS[number]
        p, q = ("z", "y") if order else ("y", "z")
        straight = shared and phase == 1
        far = phase == 3 or (step == sizes[p if phase == 1 else q] // 2 and not straight)
        half = (1 - way) // 2
        origin = -way * (step if arriving else 0 if straight else step - 1)
        at = {p: slice(None), q: homes[q]}
        lines, cols = slice(None), pl.ds(first, width)
        if phase == 1:
            at[p] = wrapped(homes[p] + origin, sizes[p])
            if far:
                lines = pl.ds(half * 16, 16)
        else:
            at[q] = wrapped(homes[q] + (origin if phase == 2 else offset), sizes[q])
            if far:
                at[p] = pl.ds(half * (sizes[p] // 2), sizes[p] // 2)
        if shared:
            side = 1 - parity if phase == 3 and arriving else parity
            cols = pl.ds(pl.multiple_of(first + side * LANES, LANES), LANES)
        return w.at[at["z"], at["y"], lines, cols]

    def gather_copy(key):
        number, phase, _, way, step = key
        axis = table[key][0][0]
        ahead = way * (step if WINDOWS[number][4] and phase == 1 else 1)
        target = {
            "y": lambda: {"sp": at_y(ahead)},
            "z": lambda: {"sp": at_z(ahead)},
            "x": lambda: {"fs": wrapped(x + ahead, X_RING)},
        }[axis]()
        ref = region(key, False)
        return pltpu.make_async_remote_copy(
            src_ref=ref, dst_ref=ref, send_sem=ring_send.at[send_at[sends[key]]],
            recv_sem=ring_recv.at[recv_at[recvs[key]]], device_id=target, device_id_type=MESH,
        )

    def block_of(number, phase, what):
        _, order, first, width, shared, _ = WINDOWS[number]
        cols = slice(first, first + (LANES if shared else width))
        if phase == 3:
            return w.at[:, :, :, cols]
        along_y = (phase == 1) == (order == 0)
        size = (ny if along_y else nz) - 1
        other = slice(None) if phase == 2 else 0
        some = slice(0, size) if what == "all" else 0
        return w.at[other, some, :, cols] if along_y else w.at[some, other, :, cols]

    def wait_for(ref, sem):
        pltpu.make_async_copy(ref, ref, sem).wait()

    def arrived(group):
        sem = ring_recv.at[recv_at[group]]
        wait_for(block_of(*group) if len(group) == 3 else region(group, True), sem)

    def prepare():
        for copy in small:
            copy.wait()
        lane = lax.broadcasted_iota(jnp.int32, (HEAD, LANES), 1)
        for k in range(rnn // LANES):
            for side, mix in enumerate((rmix, imix)):
                both = jnp.concatenate(
                    [mix[2 * k].astype(F32), mix[2 * k + 1].astype(F32)], axis=1
                )
                cols = slice(side * LANES, (side + 1) * LANES)
                bd[k, 0:HEAD, cols] = jnp.where(lane < HEAD, both, 0.0).astype(BF16)
                bd[k, HEAD:LANES, cols] = jnp.where(lane < HEAD, 0.0, both).astype(BF16)
        soft[...] = log1p_of_exp(-lrate[...]) * (-SHARPNESS)
        shift_t[...] = shift[...].T

    def normalize(first, last):
        def body(i, carry):
            at = pl.ds(pl.multiple_of(i * REACH, REACH), REACH)
            x = tok[at, :].astype(F32)
            mean = jnp.sum(x * x, axis=1, keepdims=True) * (1.0 / depth)
            keep = jnp.where(jnp.logical_and(i == 0, sp == 0), 0.0, 1.0)
            nrm[at, :] = (x * lax.rsqrt(mean + EPSILON) * gain[...] * keep).astype(BF16)
            return carry
        lax.fori_loop(first, last, body, 0, unroll=3)

    def project(first, width):
        weight = w[:, :, :, first:first + width].reshape(depth, width)
        result = jnp.dot(nrm[...], weight, preferred_element_type=F32)
        proj[:, first:first + width] = result.astype(BF16).astype(F32)

    def gates(begin, end):
        low = lax.broadcasted_iota(jnp.int32, (seg, LANES), 1) < HEAD

        def body(i, carry):
            first = pl.multiple_of(i * seg, seg)
            at = pl.ds(first, seg)
            for k in range(rnn // LANES):
                cols = slice(k * LANES, (k + 1) * LANES)
                v = proj[pl.ds(first, seg + REACH), cols]
                conv = taps[0:1, cols] * v[13:13 + seg]
                for tap in (1, 2, 3):
                    conv = conv + taps[tap:tap + 1, cols] * v[13 + tap:13 + tap + seg]
                conv = conv.astype(BF16)
                terms = jnp.dot(conv, bd[k], preferred_element_type=F32)
                rate = jax.nn.sigmoid(terms[:, :LANES])
                entry = jax.nn.sigmoid(terms[:, LANES:])
                shifts = jnp.where(
                    low, shift_t[at, 2 * k:2 * k + 1], shift_t[at, 2 * k + 1:2 * k + 2]
                )
                log_decay = rate * soft[0:1, cols] + shifts
                put = pl.ds(pl.multiple_of(i * PITCH, 8), seg)
                decay = jnp.exp(log_decay)
                aa[k, put, :] = decay
                bb[k, put, :] = (
                    jnp.sqrt(one_minus_square(decay, log_decay)) * entry * conv.astype(F32)
                )
            return carry
        lax.fori_loop(begin, end, body, 0)

    def scan():
        tiles = range(rnn // LANES)

        def body(j, carry):
            at = pl.ds(j, SEGMENTS, stride=PITCH)
            result = []
            for k in tiles:
                decay, state = carry[k]
                a, b = aa[k, at, :], bb[k, at, :]
                decay = decay * a
                state = a * state + b
                aa[k, at, :] = decay
                bb[k, at, :] = state
                result.append((decay, state))
            return tuple(result)
        start = (jnp.ones((SEGMENTS, LANES), F32), jnp.zeros((SEGMENTS, LANES), F32))
        for k, (decay, state) in enumerate(lax.fori_loop(0, seg, body, (start,) * len(tiles))):
            ends_a[:, k * LANES:(k + 1) * LANES] = decay
            ends_b[:, k * LANES:(k + 1) * LANES] = state
        total_a, total_b = jnp.ones((1, rnn), F32), jnp.zeros((1, rnn), F32)
        for s in range(SEGMENTS):
            enter[s, :, 0:rnn] = total_a
            enter[s, :, rnn:] = total_b
            a, b = ends_a[s:s + 1, :], ends_b[s:s + 1, :]
            total_a, total_b = total_a * a, a * total_b + b
        ybuf[y, :, 0:rnn] = total_a
        ybuf[y, :, rnn:] = total_b

    def sums_to_others(buf, home, n, sem, target):
        for k in range(1, n):
            pltpu.make_async_remote_copy(
                src_ref=buf.at[home], dst_ref=buf.at[home], send_sem=sem.at[0],
                recv_sem=sem.at[1], device_id={"sp": target(k)}, device_id_type=MESH,
            ).start()

    def chained(buf, n, home):
        whole = before = (jnp.ones((1, rnn), F32), jnp.zeros((1, rnn), F32))
        for s in range(n):
            a, b = buf[s, :, 0:rnn], buf[s, :, rnn:]
            before = tuple(jnp.where(s == home, new, old) for new, old in zip(whole, before))
            whole = (whole[0] * a, a * whole[1] + b)
        return whole, before

    def turned(first):
        return pl.ds(pl.multiple_of(lax.rem(first + (1 - tp) * half, rows), REACH), seg)

    def pool():
        def body(i, carry):
            first = pl.multiple_of(i * seg, seg)
            at = turned(first)
            place = sp * rows + first + lax.broadcasted_iota(jnp.int32, (seg, LANES), 0)
            for g in (0, 1):
                x = proj[pl.ds(first, seg + REACH), POOL + g * LANES:POOL + (g + 1) * LANES]
                near = x + pltpu.roll(x, 1, 0)
                if g == 1:
                    near = near + pltpu.roll(near, 2, 0)
                far = near
                for width in ((2, 4) if g == 0 else (4, 8)):
                    far = far + pltpu.roll(far, width, 0)
                window = jnp.where(tp == 0, 2 << g, 8 << g)
                summed = jnp.where(tp == 0, near, far)[REACH:]
                counts = jnp.minimum(place + 1, window).astype(F32)
                pooled = (summed / counts - x[REACH:]).astype(BF16)
                mixed = jnp.dot(pooled, pmix[g], preferred_element_type=F32)
                cols = slice(g * LANES, (g + 1) * LANES)
                acts[at, rnn + g * LANES:rnn + (g + 1) * LANES] = (
                    mixed * avg[0:1, cols]
                ).astype(BF16)
            return carry
        lax.fori_loop(0, SEGMENTS, body, 0)

    def gelu():
        scale = math.sqrt(2.0 / math.pi)

        def body(i, carry):
            at = pl.ds(pl.multiple_of(REACH + i * seg, REACH), seg)
            cols = slice(GATE, POOL)
            v = proj[at, cols]
            proj[at, cols] = v * (0.5 * (1.0 + jnp.tanh(scale * (v + 0.044715 * (v * v * v)))))
            return carry
        lax.fori_loop(0, SEGMENTS, body, 0)

    def carry_in():
        _, rows_before = chained(zbuf, nz, z)
        _, in_row = chained(ybuf, ny, y)
        entry = rows_before[0] * init[...] + rows_before[1]
        carried[...] = in_row[0] * entry + in_row[1]

    def row_total():
        whole, _ = chained(ybuf, ny, y)
        zbuf[z, :, 0:rnn] = whole[0]
        zbuf[z, :, rnn:] = whole[1]

    def finish():
        def body(i, carry):
            first = pl.multiple_of(i * seg, seg)
            at = pl.ds(pl.multiple_of(i * PITCH, 8), seg)
            put = turned(first)
            begin = enter[i, :, 0:rnn] * carried[...] + enter[i, :, rnn:]
            for k in range(rnn // LANES):
                cols = slice(k * LANES, (k + 1) * LANES)
                state = bb[k, at, :] + aa[k, at, :] * begin[:, cols]
                gate = proj[pl.ds(pl.multiple_of(REACH + first, REACH), seg),
                            GATE + k * LANES:GATE + (k + 1) * LANES]
                acts[put, cols] = (gate * state).astype(BF16)
            return carry
        lax.fori_loop(0, SEGMENTS, body, 0)

    features = ny * w.shape[2]

    def part_copy(n):
        return pltpu.make_async_remote_copy(
            src_ref=psend.at[n], dst_ref=precv.at[n], send_sem=part_send,
            recv_sem=part_recv.at[n], device_id={"tp": 1 - tp}, device_id_type=MESH,
        )

    def products():
        def body(n, carry):
            weight = w[pl.ds(2 * n, 2), :, :, OUT:PACKED].reshape(2 * features, PACKED - OUT)
            result = lax.dot_general(
                acts[...], weight, (((1,), (1,)), ((), ())), preferred_element_type=F32
            )
            for side in (0, 1):
                part = result[:, side * features:(side + 1) * features]
                psend[2 * n + side] = part[:half].astype(BF16)
                part_copy(2 * n + side).start()
                own[2 * n + side] = part[half:]
            return carry
        lax.fori_loop(0, nz // 2, body, 0)

    def out_copy(n):
        return pltpu.make_async_copy(
            obuf.at[n], out.at[:, pl.ds(pl.multiple_of(n * features, LANES), features)],
            out_sem,
        )

    def totals():
        def body(n, carry):
            part_copy(n).wait_recv()
            obuf[n] = (own[n] + precv[n].astype(F32)).astype(BF16)
            out_copy(n).start()
            return carry
        lax.fori_loop(0, nz, body, 0)

    copies = {"pair": (None, 0, ()), "halo": (None, 0, ("pair", "own"))}
    copies.update({"y_sums": (None, 0, ("scan",)), "z_sums": (None, 0, ("row_total",))})
    copies.update(table)
    blocks = (rows + REACH) // REACH
    cuts = [blocks * k // 4 // 3 * 3 for k in range(4)] + [blocks]
    normed = tuple(f"norm{k}" for k in range(4))
    pieces = {"own": (0.0, own_tokens.wait, ()), "prepare": (0.3, prepare, ())}
    for k in range(4):
        pieces[normed[k]] = (
            0.8, functools.partial(normalize, cuts[k], cuts[k + 1]), ("halo",)
        )
    pieces["value"] = (
        1.4, functools.partial(project, VALUE, GATE), complete["value"] + normed
    )
    for k in range(4):
        pieces[f"gates{k}"] = (
            0.65, functools.partial(gates, 2 * k, 2 * k + 2), ("value", "prepare")
        )
    pieces["scan"] = (0.9, scan, tuple(f"gates{k}" for k in range(4)))
    pieces["row_total"] = (0.1, row_total, ("y_sums",))
    pieces["carry_in"] = (0.1, carry_in, ("z_sums",))
    pieces["gate"] = (
        1.4, functools.partial(project, GATE, POOL - GATE), complete["gate"] + normed
    )
    pieces["project_pool"] = (0.8, functools.partial(project, POOL, OUT - POOL), complete["pool"] + normed)
    pieces["gelu"] = (0.4, gelu, ("gate",))
    pieces["pool"] = (1.4, pool, ("project_pool", "prepare"))
    pieces["finish"] = (0.3, finish, ("carry_in", "gelu"))
    pieces["products"] = (2.5, products, ("finish", "pool") + complete["out"])
    pieces["totals"] = (1.5, totals, ("products",))

    def start(key):
        if key == "pair":
            pair.start()
        elif key == "halo":
            halo.start()
        elif key == "y_sums":
            sums_to_others(ybuf, y, ny, y_sem, at_y)
        elif key == "z_sums":
            sums_to_others(zbuf, z, nz, z_sem, at_z)
        else:
            gather_copy(key).start()

    def wait(group):
        if group == "pair":
            pair.wait_recv()
        elif group == "halo":
            halo.wait_recv()
        elif group == "y_sums":
            wait_for(ybuf.at[0:ny - 1], y_sem.at[1])
        elif group == "z_sums":
            wait_for(zbuf.at[0:nz - 1], z_sem.at[1])
        else:
            arrived(group)

    waited = set()

    def settle(keys):
        for key in keys:
            group = recvs.get(key, key)
            if key in copies and group not in waited:
                waited.add(group)
                wait(group)

    for key in planned(copies, {k: (v[0], v[2]) for k, v in pieces.items()}):
        if key in copies:
            settle(copies[key][-1])
            start(key)
        else:
            settle(pieces[key][-1])
            pieces[key][1]()
    settle(copies)

    for group, k in send_at.items():
        wait_for(block_of(*group, "all"), ring_send.at[k])
    pair.wait_send()
    halo.wait_send()
    wait_for(ybuf.at[0:ny - 1], y_sem.at[0])
    wait_for(zbuf.at[0:nz - 1], z_sem.at[0])
    wait_for(psend, part_send)
    wait_for(obuf, out_sem)


def shards(ny, nz, tokens, norm_gain, pool_in, gate_in, value_in, pool_mix, averaging_factor,
           conv_taps, rate_mix, input_mix, log_rate, decay_shift, initial_state, out_pool,
           out_rnn):
    half, depth = tokens.shape
    rows = 2 * half
    rnn = log_rate.shape[0]
    lines = pool_in.shape[0]
    features = ny * lines
    sends, recvs = semaphores_of(transfers_of(ny, nz, lines)[0], ny, nz)
    dma = pltpu.SemaphoreType.DMA
    vmem = pltpu.VMEM
    scratch = [
        vmem((nz, ny, lines, PACKED), BF16),
        vmem((rows + REACH, depth), BF16),
        vmem((rows + REACH, depth), BF16),
        vmem((rows + REACH, OUT), F32),
        vmem((rnn // LANES, SEGMENTS * PITCH, LANES), F32),
        vmem((rnn // LANES, SEGMENTS * PITCH, LANES), F32),
        vmem((rows, PACKED - OUT), BF16),
        vmem((rows, rnn // HEAD), F32),
        vmem((1, depth), F32),
        vmem(pool_mix.shape, BF16),
        vmem((1, 2 * LANES), F32),
        vmem(conv_taps.shape, F32),
        vmem(rate_mix.shape, BF16),
        vmem(input_mix.shape, BF16),
        vmem((1, rnn), F32),
        vmem(decay_shift.shape, F32),
        vmem((1, rnn), F32),
        vmem((rnn // LANES, LANES, 2 * LANES), BF16),
        vmem((1, rnn), F32),
        vmem((SEGMENTS, rnn), F32),
        vmem((SEGMENTS, rnn), F32),
        vmem((SEGMENTS, 1, 2 * rnn), F32),
        vmem((1, rnn), F32),
        vmem((ny, 1, 2 * rnn), F32),
        vmem((nz, 1, 2 * rnn), F32),
        vmem((nz, half, features), BF16),
        vmem((nz, half, features), BF16),
        vmem((nz, half, features), F32),
        vmem((nz, half, features), BF16),
        dma((18,)),
        dma((len(set(sends.values())),)),
        dma((len(set(recvs.values())),)),
        dma, dma, dma, dma,
        dma((2,)), dma((2,)), dma, dma((nz,)), dma,
    ]
    anywhere = pl.BlockSpec(memory_space=pl.ANY)
    return pl.pallas_call(
        functools.partial(kernel, ny, nz),
        out_shape=jax.ShapeDtypeStruct((half, depth), BF16),
        in_specs=[anywhere] * 15,
        out_specs=anywhere,
        scratch_shapes=scratch,
        compiler_params=pltpu.CompilerParams(
            collective_id=0, has_side_effects=True, vmem_limit_bytes=56 * 1024 * 1024
        ),
        name="layer",
    )(tokens, norm_gain[None], pool_in, gate_in, value_in, pool_mix, averaging_factor[None],
      conv_taps, rate_mix, input_mix, log_rate[None], decay_shift, initial_state[None], out_pool,
      out_rnn)


def grid_of(count):
    ny = 1
    while ny * ny < count:
        ny *= 2
    return ny, count // ny


def solution(mesh):
    ny, nz = grid_of(mesh.shape["sp"])
    placed = (
        P(("fs", "sp", "tp"), None),
        P(),
        P("sp", "tp"),
        P("sp", "tp"),
        P("sp", "tp"),
        P("tp", None, None),
        P("tp"),
        P(None, "tp"),
        P("tp", None, None),
        P("tp", None, None),
        P("tp"),
        P(("fs", "tp"), "sp"),
        P(("fs", "tp")),
        P("sp", "tp"),
        P("sp", "tp"),
    )
    return jax.shard_map(
        functools.partial(shards, ny, nz), mesh=mesh, in_specs=placed,
        out_specs=P(("fs", "sp", "tp"), None), check_vma=False,
    )
```

```python
import functools
import math

import jax
import jax.numpy as jnp
from jax import lax
from jax.experimental import pallas as pl
from jax.experimental.pallas import tpu as pltpu
from jax.sharding import PartitionSpec as P

HEAD = 64
LANES = 128
REACH = 16
SEGMENTS = 8
EPSILON = 1e-06
SHARPNESS = 8.0
MESH = pl.DeviceIdType.MESH
F32 = jnp.float32
BF16 = jnp.bfloat16

VALUE = 0
GATE = 512
POOL = 1024
OUT = 1280
PACKED = 2048
PITCH = 72
WINDOWS = (
    ("value", 0, 0, 256, True, None),
    ("gate", 0, GATE, 256, True, 1),
    ("gate", 1, GATE + 384, 128, False, None),
    ("gate", 0, GATE + 256, 128, False, 1),
    ("value", 1, 256, 256, True, None),
    ("pool", 1, POOL, 256, True, 2),
    ("out", 0, OUT, 128, False, 3),
    ("out", 0, OUT + 128, 256, False, 2),
    ("out", 1, OUT + 384, 256, False, 3),
    ("out", 1, OUT + 640, 128, False, None),
)
X_RING = 4
LINK_RATE = 44e3
HOP = 2.2


def transfers_of(ny, nz, lines):
    table, complete = {}, {}

    def ring(head, axis, n, size, before):
        reached = {0: tuple(before)}
        for way in (1, -1):
            last = tuple(before)
            for step in range(1, n // 2 + 1):
                key = (*head, way, step)
                far = step == n // 2
                table[key] = ((axis, way), size // 2 if far else size, last)
                offset = n // 2 if far else -way * step
                reached[offset] = reached.get(offset, ()) + (key,)
                last = (key,)
        return reached

    def straight(head, axis, n, size):
        reached = {0: ()}
        for step in range(1, n // 2 + 1):
            for way in (1, -1) if step < n // 2 else (1,):
                key = (*head, way, step)
                table[key] = ((axis, way), size * step, ())
                reached[-way * step] = (key,)
        return reached

    for number, (name, order, _, width, shared, hold) in enumerate(WINDOWS):
        (p, np_), (q, nq) = (("y", ny), ("z", nz))[:: -1 if order else 1]
        size = lines * (width // 2 if shared else width) * 2
        first = straight((number, 1, 0), p, np_, size) if shared else ring(
            (number, 1, 0), p, np_, size, ()
        )
        row = tuple(key for keys in first.values() for key in keys)
        second = ring((number, 2, 0), q, nq, size * np_, row)
        second[0] = row
        if hold is not None:
            leader = [w[:2] for w in WINDOWS].index(("value", order))
            for way in (1, -1):
                link, size_, before = table[number, 2, 0, way, 1]
                sent = ("sent", (leader, 2, 0, way, min(hold, nq // 2)))
                table[number, 2, 0, way, 1] = (link, size_, before + (sent,))
        keys = set(row).union(*second.values())
        if shared:
            for offset in sorted(second, key=lambda o: (abs(o), o)):
                for way in (1, -1):
                    key = (number, 3, offset, way, 1)
                    table[key] = (("x", way), size * np_ // 2, second[offset])
                    keys.add(key)
        complete[name] = complete.get(name, ()) + tuple(k for k in table if k in keys)
    return table, complete


def semaphores_of(table, ny, nz):
    sends, recvs = {}, {}
    for key in table:
        number, phase, _, _, step = key
        order, shared = WINDOWS[number][1], WINDOWS[number][4]
        n = (ny, nz)[(phase - 1) ^ order] if phase < 3 else 0
        together = phase == 3 or (shared and phase == 1) or step == n // 2
        recvs[key] = (number, phase, "all" if phase == 3 or (shared and phase == 1) else "far") \
            if together else key
        sends[key] = (number, phase)
    return sends, recvs


def planned(transfers, tasks):
    clock, free, at, order = 0.0, {}, {}, []
    copies, pieces = dict(transfers), dict(tasks)
    never = 1e9

    def first_ready(table):
        for key, entry in table.items():
            if all(at.get(other, never) <= clock for other in entry[-1]):
                return key
        return None

    while copies or pieces:
        key = first_ready(copies)
        if key is not None:
            link, size, _ = copies.pop(key)
            begin = max(clock, free.get(link, 0.0)) if link else clock
            free[link] = begin + size / LINK_RATE
            at[key] = free[link] + HOP * (1 if link else 2)
            at["sent", key] = clock
            clock += 0.02
            order.append(key)
            continue
        key = first_ready(pieces)
        if key is not None:
            cost, _ = pieces.pop(key)
            clock += cost
            at[key] = clock
            order.append(key)
            continue
        clock = min(time for time in at.values() if time > clock)
    return order


def wrapped(index, count):
    return lax.rem(index + count, count)


def log1p_of_exp(v):
    e = jnp.exp(-jnp.abs(v))
    s = e / (2.0 + e)
    q = s * s
    total = jnp.full_like(q, 1.0 / 15.0)
    for odd in (13, 11, 9, 7, 5, 3, 1):
        total = total * q + 1.0 / odd
    return jnp.maximum(v, 0.0) + 2.0 * s * total


def one_minus_square(a, x):
    v = 2.0 * x
    series = jnp.full_like(v, 1.0 / 720.0)
    for k in (120.0, 24.0, 6.0, 2.0, 1.0):
        series = series * v + 1.0 / k
    return jnp.where(v > -0.25, -v * series, 1.0 - a * a)


def kernel(ny, nz, *refs):
    (tok_in, gain_in, pool_in, gate_in, value_in, pmix_in, avg_in, taps_in, rmix_in, imix_in,
     lrate_in, shift_in, init_in, opool_in, ornn_in, own, precv,
     w, tok, nrm, proj, aa, bb, acts, shift_t, gain, pmix, avg, taps, rmix, imix, lrate, shift,
     init, bd, soft, ends_a, ends_b, enter, carried, ybuf, zbuf, psend,
     local_sem, ring_send, ring_recv, pair_send, pair_recv, next_send, next_recv,
     y_sem, z_sem, part_send, part_recv) = refs
    half, depth = tok_in.shape
    rows = 2 * half
    seg = rows // SEGMENTS
    rnn = lrate.shape[1]
    sp, tp = lax.axis_index("sp"), lax.axis_index("tp")
    z, y, x = sp // ny, lax.rem(sp, ny), lax.axis_index("fs")
    count = ny * nz

    def at_y(k):
        return z * ny + wrapped(y + k, ny)

    def at_z(k):
        return wrapped(z + k, nz) * ny + y

    def local(k, src, dst):
        return pltpu.make_async_copy(src, dst, local_sem.at[k])

    mine = w.at[z, y]
    parity = lax.rem(x, 2)
    sources = {"value": (value_in, 0), "gate": (gate_in, GATE), "pool": (pool_in, POOL)}
    packing = []
    for name, _, first, width, shared, _ in WINDOWS:
        if name in sources:
            src, base = sources[name]
            if shared:
                skip, width = pl.multiple_of(parity * LANES, LANES), width // 2
                cols, from_ = pl.ds(first + skip, width), pl.ds(first - base + skip, width)
            else:
                cols, from_ = pl.ds(first, width), pl.ds(first - base, width)
            packing.append(local(len(packing), src.at[:, from_], mine.at[:, cols]))
    packing.append(local(len(packing), ornn_in, mine.at[:, OUT:OUT + rnn]))
    packing.append(local(len(packing), opool_in, mine.at[:, OUT + rnn:PACKED]))
    my_rows = pl.ds(pl.multiple_of(REACH + tp * half, REACH), half)
    own_tokens = local(8, tok_in, tok.at[my_rows])
    small = [
        local(9 + k, src, dst)
        for k, (src, dst) in enumerate(
            [(gain_in, gain), (pmix_in, pmix), (avg_in, avg), (taps_in, taps), (rmix_in, rmix),
             (imix_in, imix), (lrate_in, lrate), (shift_in, shift), (init_in, init)]
        )
    ]
    for copy in packing + [own_tokens] + small:
        copy.start()

    barrier = pltpu.get_barrier_semaphore()
    peers = [at_y(k) for k in range(1, ny)] + [at_z(k) for k in range(1, nz)]
    peers += [wrapped(sp + 1, count), wrapped(sp - 1, count)]
    for peer in peers:
        pl.semaphore_signal(barrier, inc=1, device_id={"sp": peer}, device_id_type=MESH)
    pl.semaphore_signal(barrier, inc=1, device_id={"tp": 1 - tp}, device_id_type=MESH)
    for way in (1, -1):
        pl.semaphore_signal(
            barrier, inc=1, device_id={"fs": wrapped(x + way, X_RING)}, device_id_type=MESH
        )
    for copy in packing:
        copy.wait()
    pl.semaphore_wait(barrier, len(peers) + 3)

    pair = pltpu.make_async_remote_copy(
        src_ref=tok_in, dst_ref=tok.at[my_rows], send_sem=pair_send, recv_sem=pair_recv,
        device_id={"tp": 1 - tp}, device_id_type=MESH,
    )
    halo = pltpu.make_async_remote_copy(
        src_ref=tok.at[pl.ds(rows, REACH)], dst_ref=tok.at[pl.ds(0, REACH)],
        send_sem=next_send, recv_sem=next_recv,
        device_id={"sp": wrapped(sp + 1, count)}, device_id_type=MESH,
    )

    table, complete = transfers_of(ny, nz, w.shape[2])
    sends, recvs = semaphores_of(table, ny, nz)
    send_at = {group: k for k, group in enumerate(dict.fromkeys(sends.values()))}
    recv_at = {group: k for k, group in enumerate(dict.fromkeys(recvs.values()))}
    sizes = {"y": ny, "z": nz}
    homes = {"y": y, "z": z}

    def region(key, arriving):
        number, phase, offset, way, step = key
        _, order, first, width, shared, _ = WINDOWS[number]
        p, q = ("z", "y") if order else ("y", "z")
        straight = shared and phase == 1
        far = phase == 3 or (step == sizes[p if phase == 1 else q] // 2 and not straight)
        half = (1 - way) // 2
        origin = -way * (step if arriving else 0 if straight else step - 1)
        at = {p: slice(None), q: homes[q]}
        lines, cols = slice(None), pl.ds(first, width)
        if phase == 1:
            at[p] = wrapped(homes[p] + origin, sizes[p])
            if far:
                lines = pl.ds(half * 16, 16)
        else:
            at[q] = wrapped(homes[q] + (origin if phase == 2 else offset), sizes[q])
            if far:
                at[p] = pl.ds(half * (sizes[p] // 2), sizes[p] // 2)
        if shared:
            side = 1 - parity if phase == 3 and arriving else parity
            cols = pl.ds(pl.multiple_of(first + side * LANES, LANES), LANES)
        return w.at[at["z"], at["y"], lines, cols]

    def gather_copy(key):
        number, phase, _, way, step = key
        axis = table[key][0][0]
        ahead = way * (step if WINDOWS[number][4] and phase == 1 else 1)
        target = {
            "y": lambda: {"sp": at_y(ahead)},
            "z": lambda: {"sp": at_z(ahead)},
            "x": lambda: {"fs": wrapped(x + ahead, X_RING)},
        }[axis]()
        ref = region(key, False)
        return pltpu.make_async_remote_copy(
            src_ref=ref, dst_ref=ref, send_sem=ring_send.at[send_at[sends[key]]],
            recv_sem=ring_recv.at[recv_at[recvs[key]]], device_id=target, device_id_type=MESH,
        )

    def block_of(number, phase, what):
        _, order, first, width, shared, _ = WINDOWS[number]
        cols = slice(first, first + (LANES if shared else width))
        if phase == 3:
            return w.at[:, :, :, cols]
        along_y = (phase == 1) == (order == 0)
        size = (ny if along_y else nz) - 1
        other = slice(None) if phase == 2 else 0
        some = slice(0, size) if what == "all" else 0
        return w.at[other, some, :, cols] if along_y else w.at[some, other, :, cols]

    def wait_for(ref, sem):
        pltpu.make_async_copy(ref, ref, sem).wait()

    def arrived(group):
        sem = ring_recv.at[recv_at[group]]
        wait_for(block_of(*group) if len(group) == 3 else region(group, True), sem)

    def prepare():
        for copy in small:
            copy.wait()
        lane = lax.broadcasted_iota(jnp.int32, (HEAD, LANES), 1)
        for k in range(rnn // LANES):
            for side, mix in enumerate((rmix, imix)):
                both = jnp.concatenate(
                    [mix[2 * k].astype(F32), mix[2 * k + 1].astype(F32)], axis=1
                )
                cols = slice(side * LANES, (side + 1) * LANES)
                bd[k, 0:HEAD, cols] = jnp.where(lane < HEAD, both, 0.0).astype(BF16)
                bd[k, HEAD:LANES, cols] = jnp.where(lane < HEAD, 0.0, both).astype(BF16)
        soft[...] = log1p_of_exp(-lrate[...]) * (-SHARPNESS)
        shift_t[...] = shift[...].T

    def normalize(first, last):
        def body(i, carry):
            at = pl.ds(pl.multiple_of(i * REACH, REACH), REACH)
            x = tok[at, :].astype(F32)
            mean = jnp.sum(x * x, axis=1, keepdims=True) * (1.0 / depth)
            keep = jnp.where(jnp.logical_and(i == 0, sp == 0), 0.0, 1.0)
            nrm[at, :] = (x * lax.rsqrt(mean + EPSILON) * gain[...] * keep).astype(BF16)
            return carry
        lax.fori_loop(first, last, body, 0, unroll=3)

    def project(first, width):
        weight = w[:, :, :, first:first + width].reshape(depth, width)
        result = jnp.dot(nrm[...], weight, preferred_element_type=F32)
        proj[:, first:first + width] = result.astype(BF16).astype(F32)

    def gates(begin, end):
        low = lax.broadcasted_iota(jnp.int32, (seg, LANES), 1) < HEAD

        def body(i, carry):
            first = pl.multiple_of(i * seg, seg)
            at = pl.ds(first, seg)
            for k in range(rnn // LANES):
                cols = slice(k * LANES, (k + 1) * LANES)
                v = proj[pl.ds(first, seg + REACH), cols]
                conv = taps[0:1, cols] * v[13:13 + seg]
                for tap in (1, 2, 3):
                    conv = conv + taps[tap:tap + 1, cols] * v[13 + tap:13 + tap + seg]
                conv = conv.astype(BF16)
                terms = jnp.dot(conv, bd[k], preferred_element_type=F32)
                rate = jax.nn.sigmoid(terms[:, :LANES])
                entry = jax.nn.sigmoid(terms[:, LANES:])
                shifts = jnp.where(
                    low, shift_t[at, 2 * k:2 * k + 1], shift_t[at, 2 * k + 1:2 * k + 2]
                )
                log_decay = rate * soft[0:1, cols] + shifts
                put = pl.ds(pl.multiple_of(i * PITCH, 8), seg)
                decay = jnp.exp(log_decay)
                aa[k, put, :] = decay
                bb[k, put, :] = (
                    jnp.sqrt(one_minus_square(decay, log_decay)) * entry * conv.astype(F32)
                )
            return carry
        lax.fori_loop(begin, end, body, 0)

    def scan():
        tiles = range(rnn // LANES)

        def body(j, carry):
            at = pl.ds(j, SEGMENTS, stride=PITCH)
            result = []
            for k in tiles:
                decay, state = carry[k]
                a, b = aa[k, at, :], bb[k, at, :]
                decay = decay * a
                state = a * state + b
                aa[k, at, :] = decay
                bb[k, at, :] = state
                result.append((decay, state))
            return tuple(result)
        start = (jnp.ones((SEGMENTS, LANES), F32), jnp.zeros((SEGMENTS, LANES), F32))
        for k, (decay, state) in enumerate(lax.fori_loop(0, seg, body, (start,) * len(tiles))):
            ends_a[:, k * LANES:(k + 1) * LANES] = decay
            ends_b[:, k * LANES:(k + 1) * LANES] = state
        total_a, total_b = jnp.ones((1, rnn), F32), jnp.zeros((1, rnn), F32)
        for s in range(SEGMENTS):
            enter[s, :, 0:rnn] = total_a
            enter[s, :, rnn:] = total_b
            a, b = ends_a[s:s + 1, :], ends_b[s:s + 1, :]
            total_a, total_b = total_a * a, a * total_b + b
        ybuf[y, :, 0:rnn] = total_a
        ybuf[y, :, rnn:] = total_b

    def sums_to_others(buf, home, n, sem, target):
        for k in range(1, n):
            pltpu.make_async_remote_copy(
                src_ref=buf.at[home], dst_ref=buf.at[home], send_sem=sem.at[0],
                recv_sem=sem.at[1], device_id={"sp": target(k)}, device_id_type=MESH,
            ).start()

    def chained(buf, n, home):
        whole = before = (jnp.ones((1, rnn), F32), jnp.zeros((1, rnn), F32))
        for s in range(n):
            a, b = buf[s, :, 0:rnn], buf[s, :, rnn:]
            before = tuple(jnp.where(s == home, new, old) for new, old in zip(whole, before))
            whole = (whole[0] * a, a * whole[1] + b)
        return whole, before

    def turned(first):
        return pl.ds(pl.multiple_of(lax.rem(first + (1 - tp) * half, rows), REACH), seg)

    def pool():
        def body(i, carry):
            first = pl.multiple_of(i * seg, seg)
            at = turned(first)
            place = sp * rows + first + lax.broadcasted_iota(jnp.int32, (seg, LANES), 0)
            for g in (0, 1):
                x = proj[pl.ds(first, seg + REACH), POOL + g * LANES:POOL + (g + 1) * LANES]
                near = x + pltpu.roll(x, 1, 0)
                if g == 1:
                    near = near + pltpu.roll(near, 2, 0)
                far = near
                for width in ((2, 4) if g == 0 else (4, 8)):
                    far = far + pltpu.roll(far, width, 0)
                window = jnp.where(tp == 0, 2 << g, 8 << g)
                summed = jnp.where(tp == 0, near, far)[REACH:]
                counts = jnp.minimum(place + 1, window).astype(F32)
                pooled = (summed / counts - x[REACH:]).astype(BF16)
                mixed = jnp.dot(pooled, pmix[g], preferred_element_type=F32)
                cols = slice(g * LANES, (g + 1) * LANES)
                acts[at, rnn + g * LANES:rnn + (g + 1) * LANES] = (
                    mixed * avg[0:1, cols]
                ).astype(BF16)
            return carry
        lax.fori_loop(0, SEGMENTS, body, 0)

    def gelu():
        scale = math.sqrt(2.0 / math.pi)

        def body(i, carry):
            at = pl.ds(pl.multiple_of(REACH + i * seg, REACH), seg)
            cols = slice(GATE, POOL)
            v = proj[at, cols]
            proj[at, cols] = v * (0.5 * (1.0 + jnp.tanh(scale * (v + 0.044715 * (v * v * v)))))
            return carry
        lax.fori_loop(0, SEGMENTS, body, 0)

    def carry_in():
        _, rows_before = chained(zbuf, nz, z)
        _, in_row = chained(ybuf, ny, y)
        entry = rows_before[0] * init[...] + rows_before[1]
        carried[...] = in_row[0] * entry + in_row[1]

    def row_total():
        whole, _ = chained(ybuf, ny, y)
        zbuf[z, :, 0:rnn] = whole[0]
        zbuf[z, :, rnn:] = whole[1]

    def finish():
        def body(i, carry):
            first = pl.multiple_of(i * seg, seg)
            at = pl.ds(pl.multiple_of(i * PITCH, 8), seg)
            put = turned(first)
            begin = enter[i, :, 0:rnn] * carried[...] + enter[i, :, rnn:]
            for k in range(rnn // LANES):
                cols = slice(k * LANES, (k + 1) * LANES)
                state = bb[k, at, :] + aa[k, at, :] * begin[:, cols]
                gate = proj[pl.ds(pl.multiple_of(REACH + first, REACH), seg),
                            GATE + k * LANES:GATE + (k + 1) * LANES]
                acts[put, cols] = (gate * state).astype(BF16)
            return carry
        lax.fori_loop(0, SEGMENTS, body, 0)

    features = ny * w.shape[2]

    def columns(n):
        return pl.ds(pl.multiple_of(n * features, LANES), features)

    def part_copy(n):
        return pltpu.make_async_remote_copy(
            src_ref=psend.at[n], dst_ref=precv.at[:, columns(n)], send_sem=part_send,
            recv_sem=part_recv, device_id={"tp": 1 - tp}, device_id_type=MESH,
        )

    def products():
        def body(n, carry):
            weight = w[pl.ds(2 * n, 2), :, :, OUT:PACKED].reshape(2 * features, PACKED - OUT)
            result = lax.dot_general(
                acts[...], weight, (((1,), (1,)), ((), ())), preferred_element_type=F32
            )
            for side in (0, 1):
                part = result[:, side * features:(side + 1) * features]
                psend[2 * n + side] = part[:half].astype(BF16)
                part_copy(2 * n + side).start()
                own[:, columns(2 * n + side)] = part[half:]
            return carry
        lax.fori_loop(0, nz // 2, body, 0)

    def totals():
        wait_for(precv, part_recv)

    copies = {"pair": (None, 0, ()), "halo": (None, 0, ("pair", "own"))}
    copies.update({"y_sums": (None, 0, ("scan",)), "z_sums": (None, 0, ("row_total",))})
    copies.update(table)
    blocks = (rows + REACH) // REACH
    cuts = [blocks * k // 4 // 3 * 3 for k in range(4)] + [blocks]
    normed = tuple(f"norm{k}" for k in range(4))
    pieces = {"own": (0.0, own_tokens.wait, ()), "prepare": (0.3, prepare, ())}
    for k in range(4):
        pieces[normed[k]] = (
            0.8, functools.partial(normalize, cuts[k], cuts[k + 1]), ("halo",)
        )
    pieces["value"] = (
        1.4, functools.partial(project, VALUE, GATE), complete["value"] + normed
    )
    for k in range(4):
        pieces[f"gates{k}"] = (
            0.65, functools.partial(gates, 2 * k, 2 * k + 2), ("value", "prepare")
        )
    pieces["scan"] = (0.9, scan, tuple(f"gates{k}" for k in range(4)))
    pieces["row_total"] = (0.1, row_total, ("y_sums",))
    pieces["carry_in"] = (0.1, carry_in, ("z_sums",))
    pieces["gate"] = (
        1.4, functools.partial(project, GATE, POOL - GATE), complete["gate"] + normed
    )
    pieces["project_pool"] = (0.8, functools.partial(project, POOL, OUT - POOL), complete["pool"] + normed)
    pieces["gelu"] = (0.4, gelu, ("gate",))
    pieces["pool"] = (1.4, pool, ("project_pool", "prepare"))
    pieces["finish"] = (0.3, finish, ("carry_in", "gelu"))
    pieces["products"] = (2.5, products, ("finish", "pool") + complete["out"])
    pieces["totals"] = (1.0, totals, ("products",))

    def start(key):
        if key == "pair":
            pair.start()
        elif key == "halo":
            halo.start()
        elif key == "y_sums":
            sums_to_others(ybuf, y, ny, y_sem, at_y)
        elif key == "z_sums":
            sums_to_others(zbuf, z, nz, z_sem, at_z)
        else:
            gather_copy(key).start()

    def wait(group):
        if group == "pair":
            pair.wait_recv()
        elif group == "halo":
            halo.wait_recv()
        elif group == "y_sums":
            wait_for(ybuf.at[0:ny - 1], y_sem.at[1])
        elif group == "z_sums":
            wait_for(zbuf.at[0:nz - 1], z_sem.at[1])
        else:
            arrived(group)

    waited = set()

    def settle(keys):
        for key in keys:
            group = recvs.get(key, key)
            if key in copies and group not in waited:
                waited.add(group)
                wait(group)

    for key in planned(copies, {k: (v[0], v[2]) for k, v in pieces.items()}):
        if key in copies:
            settle(copies[key][-1])
            start(key)
        else:
            settle(pieces[key][-1])
            pieces[key][1]()
    settle(copies)

    for group, k in send_at.items():
        wait_for(block_of(*group, "all"), ring_send.at[k])
    pair.wait_send()
    halo.wait_send()
    wait_for(ybuf.at[0:ny - 1], y_sem.at[0])
    wait_for(zbuf.at[0:nz - 1], z_sem.at[0])
    wait_for(psend, part_send)


def shards(ny, nz, tokens, norm_gain, pool_in, gate_in, value_in, pool_mix, averaging_factor,
           conv_taps, rate_mix, input_mix, log_rate, decay_shift, initial_state, out_pool,
           out_rnn):
    half, depth = tokens.shape
    rows = 2 * half
    rnn = log_rate.shape[0]
    lines = pool_in.shape[0]
    features = ny * lines
    sends, recvs = semaphores_of(transfers_of(ny, nz, lines)[0], ny, nz)
    dma = pltpu.SemaphoreType.DMA
    vmem = pltpu.VMEM
    scratch = [
        vmem((nz, ny, lines, PACKED), BF16),
        vmem((rows + REACH, depth), BF16),
        vmem((rows + REACH, depth), BF16),
        vmem((rows + REACH, OUT), F32),
        vmem((rnn // LANES, SEGMENTS * PITCH, LANES), F32),
        vmem((rnn // LANES, SEGMENTS * PITCH, LANES), F32),
        vmem((rows, PACKED - OUT), BF16),
        vmem((rows, rnn // HEAD), F32),
        vmem((1, depth), F32),
        vmem(pool_mix.shape, BF16),
        vmem((1, 2 * LANES), F32),
        vmem(conv_taps.shape, F32),
        vmem(rate_mix.shape, BF16),
        vmem(input_mix.shape, BF16),
        vmem((1, rnn), F32),
        vmem(decay_shift.shape, F32),
        vmem((1, rnn), F32),
        vmem((rnn // LANES, LANES, 2 * LANES), BF16),
        vmem((1, rnn), F32),
        vmem((SEGMENTS, rnn), F32),
        vmem((SEGMENTS, rnn), F32),
        vmem((SEGMENTS, 1, 2 * rnn), F32),
        vmem((1, rnn), F32),
        vmem((ny, 1, 2 * rnn), F32),
        vmem((nz, 1, 2 * rnn), F32),
        vmem((nz, half, features), BF16),
        dma((18,)),
        dma((len(set(sends.values())),)),
        dma((len(set(recvs.values())),)),
        dma, dma, dma, dma,
        dma((2,)), dma((2,)), dma, dma,
    ]
    anywhere = pl.BlockSpec(memory_space=pl.ANY)
    own, theirs = pl.pallas_call(
        functools.partial(kernel, ny, nz),
        out_shape=(vmem((half, depth), F32), vmem((half, depth), BF16)),
        in_specs=[anywhere] * 15,
        out_specs=(pl.BlockSpec(memory_space=vmem),) * 2,
        scratch_shapes=scratch,
        compiler_params=pltpu.CompilerParams(
            collective_id=0, has_side_effects=True, vmem_limit_bytes=56 * 1024 * 1024
        ),
        name="layer",
    )(tokens, norm_gain[None], pool_in, gate_in, value_in, pool_mix, averaging_factor[None],
      conv_taps, rate_mix, input_mix, log_rate[None], decay_shift, initial_state[None], out_pool,
      out_rnn)
    return (own + theirs.astype(F32)).astype(BF16)


def grid_of(count):
    ny = 1
    while ny * ny < count:
        ny *= 2
    return ny, count // ny


def solution(mesh):
    ny, nz = grid_of(mesh.shape["sp"])
    placed = (
        P(("fs", "sp", "tp"), None),
        P(),
        P("sp", "tp"),
        P("sp", "tp"),
        P("sp", "tp"),
        P("tp", None, None),
        P("tp"),
        P(None, "tp"),
        P("tp", None, None),
        P("tp", None, None),
        P("tp"),
        P(("fs", "tp"), "sp"),
        P(("fs", "tp")),
        P("sp", "tp"),
        P("sp", "tp"),
    )
    return jax.shard_map(
        functools.partial(shards, ny, nz), mesh=mesh, in_specs=placed,
        out_specs=P(("fs", "sp", "tp"), None), check_vma=False,
    )
```

```python
import functools
import math

import jax
import jax.numpy as jnp
from jax import lax
from jax.experimental import pallas as pl
from jax.experimental.pallas import tpu as pltpu
from jax.sharding import PartitionSpec as P

HEAD = 64
LANES = 128
REACH = 16
SEGMENTS = 8
EPSILON = 1e-06
SHARPNESS = 8.0
MESH = pl.DeviceIdType.MESH
F32 = jnp.float32
BF16 = jnp.bfloat16

VALUE = 0
GATE = 512
POOL = 1024
OUT = 1280
PACKED = 2048
PITCH = 72
WINDOWS = (
    ("value", 0, 0, 256, True, None),
    ("gate", 0, GATE, 256, True, 1),
    ("gate", 1, GATE + 384, 128, False, None),
    ("gate", 0, GATE + 256, 128, False, 1),
    ("value", 1, 256, 256, True, None),
    ("pool", 1, POOL, 256, True, 2),
    ("out", 0, OUT, 128, False, 3),
    ("out", 0, OUT + 128, 256, False, 2),
    ("out", 1, OUT + 384, 256, False, 3),
    ("out", 1, OUT + 640, 128, False, None),
)
X_RING = 4
LINK_RATE = 44e3
HOP = 2.6


def transfers_of(ny, nz, lines):
    table, complete = {}, {}

    def ring(head, axis, n, size, before):
        reached = {0: tuple(before)}
        for way in (1, -1):
            last = tuple(before)
            for step in range(1, n // 2 + 1):
                key = (*head, way, step)
                far = step == n // 2
                table[key] = ((axis, way), size // 2 if far else size, last)
                offset = n // 2 if far else -way * step
                reached[offset] = reached.get(offset, ()) + (key,)
                last = (key,)
        return reached

    def straight(head, axis, n, size):
        reached = {0: ()}
        for step in range(1, n // 2 + 1):
            for way in (1, -1) if step < n // 2 else (1,):
                key = (*head, way, step)
                table[key] = ((axis, way), size * step, ())
                reached[-way * step] = (key,)
        return reached

    for number, (name, order, _, width, shared, hold) in enumerate(WINDOWS):
        (p, np_), (q, nq) = (("y", ny), ("z", nz))[:: -1 if order else 1]
        size = lines * (width // 2 if shared else width) * 2
        first = straight((number, 1, 0), p, np_, size) if shared else ring(
            (number, 1, 0), p, np_, size, ()
        )
        row = tuple(key for keys in first.values() for key in keys)
        second = ring((number, 2, 0), q, nq, size * np_, row)
        second[0] = row
        if hold is not None:
            leader = [w[:2] for w in WINDOWS].index(("value", order))
            for way in (1, -1):
                link, size_, before = table[number, 2, 0, way, 1]
                sent = ("sent", (leader, 2, 0, way, min(hold, nq // 2)))
                table[number, 2, 0, way, 1] = (link, size_, before + (sent,))
        keys = set(row).union(*second.values())
        if shared:
            for offset in sorted(second, key=lambda o: (abs(o), o)):
                for way in (1, -1):
                    key = (number, 3, offset, way, 1)
                    table[key] = (("x", way), size * np_ // 2, second[offset])
                    keys.add(key)
        complete[name] = complete.get(name, ()) + tuple(k for k in table if k in keys)
    return table, complete


def semaphores_of(table, ny, nz):
    sends, recvs = {}, {}
    for key in table:
        number, phase, _, _, step = key
        order, shared = WINDOWS[number][1], WINDOWS[number][4]
        n = (ny, nz)[(phase - 1) ^ order] if phase < 3 else 0
        together = phase == 3 or (shared and phase == 1) or step == n // 2
        recvs[key] = (number, phase, "all" if phase == 3 or (shared and phase == 1) else "far") \
            if together else key
        sends[key] = (number, phase)
    return sends, recvs


def planned(transfers, tasks):
    clock, free, at, order = 0.0, {}, {}, []
    copies, pieces = dict(transfers), dict(tasks)
    never = 1e9

    def first_ready(table):
        for key, entry in table.items():
            if all(at.get(other, never) <= clock for other in entry[-1]):
                return key
        return None

    while copies or pieces:
        key = first_ready(copies)
        if key is not None:
            link, size, _ = copies.pop(key)
            begin = max(clock, free.get(link, 0.0)) if link else clock
            free[link] = begin + size / LINK_RATE
            at[key] = free[link] + HOP * (1 if link else 2)
            at["sent", key] = clock
            clock += 0.02
            order.append(key)
            continue
        key = first_ready(pieces)
        if key is not None:
            cost, _ = pieces.pop(key)
            clock += cost
            at[key] = clock
            order.append(key)
            continue
        clock = min(time for time in at.values() if time > clock)
    return order


def wrapped(index, count):
    return lax.rem(index + count, count)


def log1p_of_exp(v):
    e = jnp.exp(-jnp.abs(v))
    s = e / (2.0 + e)
    q = s * s
    total = jnp.full_like(q, 1.0 / 15.0)
    for odd in (13, 11, 9, 7, 5, 3, 1):
        total = total * q + 1.0 / odd
    return jnp.maximum(v, 0.0) + 2.0 * s * total


def one_minus_square(a, x):
    v = 2.0 * x
    series = jnp.full_like(v, 1.0 / 720.0)
    for k in (120.0, 24.0, 6.0, 2.0, 1.0):
        series = series * v + 1.0 / k
    return jnp.where(v > -0.25, -v * series, 1.0 - a * a)


def kernel(ny, nz, *refs):
    (tok_in, gain_in, pool_in, gate_in, value_in, pmix_in, avg_in, taps_in, rmix_in, imix_in,
     lrate_in, shift_in, init_in, opool_in, ornn_in, own, precv,
     w, tok, nrm, proj, aa, bb, acts, shift_t, gain, pmix, avg, taps, rmix, imix, lrate, shift,
     init, bd, soft, ends_a, ends_b, enter, carried, ybuf, zbuf, psend,
     local_sem, ring_send, ring_recv, pair_send, pair_recv, next_send, next_recv,
     y_sem, z_sem, part_send, part_recv) = refs
    half, depth = tok_in.shape
    rows = 2 * half
    seg = rows // SEGMENTS
    rnn = lrate.shape[1]
    sp, tp = lax.axis_index("sp"), lax.axis_index("tp")
    z, y, x = sp // ny, lax.rem(sp, ny), lax.axis_index("fs")
    count = ny * nz

    def at_y(k):
        return z * ny + wrapped(y + k, ny)

    def at_z(k):
        return wrapped(z + k, nz) * ny + y

    def wait_for(ref, sem):
        pltpu.make_async_copy(ref, ref, sem).wait()

    def local(k, src, dst):
        return pltpu.make_async_copy(src, dst, local_sem.at[k])

    mine = w.at[z, y]
    parity = lax.rem(x, 2)
    sources = {"value": (value_in, 0), "gate": (gate_in, GATE), "pool": (pool_in, POOL)}
    packing = []
    for name, _, first, width, shared, _ in WINDOWS:
        if name in sources:
            src, base = sources[name]
            if shared:
                skip, width = pl.multiple_of(parity * LANES, LANES), width // 2
                cols, from_ = pl.ds(first + skip, width), pl.ds(first - base + skip, width)
            else:
                cols, from_ = pl.ds(first, width), pl.ds(first - base, width)
            packing.append(local(0, src.at[:, from_], mine.at[:, cols]))
    packing.append(local(0, ornn_in, mine.at[:, OUT:OUT + rnn]))
    packing.append(local(0, opool_in, mine.at[:, OUT + rnn:PACKED]))
    my_rows = pl.ds(pl.multiple_of(REACH + tp * half, REACH), half)
    own_tokens = local(1, tok_in, tok.at[my_rows])
    small = [
        local(2 + k, src, dst)
        for k, (src, dst) in enumerate(
            [(gain_in, gain), (pmix_in, pmix), (avg_in, avg), (taps_in, taps), (rmix_in, rmix),
             (imix_in, imix), (lrate_in, lrate), (shift_in, shift), (init_in, init)]
        )
    ]
    for copy in packing + [own_tokens] + small:
        copy.start()

    barrier = pltpu.get_barrier_semaphore()
    peers = [at_y(k) for k in range(1, ny)] + [at_z(k) for k in range(1, nz)]
    peers += [wrapped(sp + 1, count), wrapped(sp - 1, count)]
    for peer in peers:
        pl.semaphore_signal(barrier, inc=1, device_id={"sp": peer}, device_id_type=MESH)
    pl.semaphore_signal(barrier, inc=1, device_id={"tp": 1 - tp}, device_id_type=MESH)
    for way in (1, -1):
        pl.semaphore_signal(
            barrier, inc=1, device_id={"fs": wrapped(x + way, X_RING)}, device_id_type=MESH
        )
    taken = PACKED - sum(width // 2 for _, _, _, width, shared, _ in WINDOWS if shared)
    wait_for(w.at[0, 0, :, 0:taken], local_sem.at[0])
    pl.semaphore_wait(barrier, len(peers) + 3)

    pair = pltpu.make_async_remote_copy(
        src_ref=tok_in, dst_ref=tok.at[my_rows], send_sem=pair_send, recv_sem=pair_recv,
        device_id={"tp": 1 - tp}, device_id_type=MESH,
    )
    halo = pltpu.make_async_remote_copy(
        src_ref=tok.at[pl.ds(rows, REACH)], dst_ref=tok.at[pl.ds(0, REACH)],
        send_sem=next_send, recv_sem=next_recv,
        device_id={"sp": wrapped(sp + 1, count)}, device_id_type=MESH,
    )

    table, complete = transfers_of(ny, nz, w.shape[2])
    sends, recvs = semaphores_of(table, ny, nz)
    send_at = {group: k for k, group in enumerate(dict.fromkeys(sends.values()))}
    recv_at = {group: k for k, group in enumerate(dict.fromkeys(recvs.values()))}
    sizes = {"y": ny, "z": nz}
    homes = {"y": y, "z": z}

    def region(key, arriving):
        number, phase, offset, way, step = key
        _, order, first, width, shared, _ = WINDOWS[number]
        p, q = ("z", "y") if order else ("y", "z")
        straight = shared and phase == 1
        far = phase == 3 or (step == sizes[p if phase == 1 else q] // 2 and not straight)
        half = (1 - way) // 2
        origin = -way * (step if arriving else 0 if straight else step - 1)
        at = {p: slice(None), q: homes[q]}
        lines, cols = slice(None), pl.ds(first, width)
        if phase == 1:
            at[p] = wrapped(homes[p] + origin, sizes[p])
            if far:
                lines = pl.ds(half * 16, 16)
        else:
            at[q] = wrapped(homes[q] + (origin if phase == 2 else offset), sizes[q])
            if far:
                at[p] = pl.ds(half * (sizes[p] // 2), sizes[p] // 2)
        if shared:
            side = 1 - parity if phase == 3 and arriving else parity
            cols = pl.ds(pl.multiple_of(first + side * LANES, LANES), LANES)
        return w.at[at["z"], at["y"], lines, cols]

    def gather_copy(key):
        number, phase, _, way, step = key
        axis = table[key][0][0]
        ahead = way * (step if WINDOWS[number][4] and phase == 1 else 1)
        target = {
            "y": lambda: {"sp": at_y(ahead)},
            "z": lambda: {"sp": at_z(ahead)},
            "x": lambda: {"fs": wrapped(x + ahead, X_RING)},
        }[axis]()
        ref = region(key, False)
        return pltpu.make_async_remote_copy(
            src_ref=ref, dst_ref=ref, send_sem=ring_send.at[send_at[sends[key]]],
            recv_sem=ring_recv.at[recv_at[recvs[key]]], device_id=target, device_id_type=MESH,
        )

    def block_of(number, phase, what):
        _, order, first, width, shared, _ = WINDOWS[number]
        cols = slice(first, first + (LANES if shared else width))
        if phase == 3:
            return w.at[:, :, :, cols]
        along_y = (phase == 1) == (order == 0)
        size = (ny if along_y else nz) - 1
        other = slice(None) if phase == 2 else 0
        some = slice(0, size) if what == "all" else 0
        return w.at[other, some, :, cols] if along_y else w.at[some, other, :, cols]

    def arrived(group):
        sem = ring_recv.at[recv_at[group]]
        wait_for(block_of(*group) if len(group) == 3 else region(group, True), sem)

    def prepare():
        for copy in small:
            copy.wait()
        lane = lax.broadcasted_iota(jnp.int32, (HEAD, LANES), 1)
        for k in range(rnn // LANES):
            for side, mix in enumerate((rmix, imix)):
                both = jnp.concatenate(
                    [mix[2 * k].astype(F32), mix[2 * k + 1].astype(F32)], axis=1
                )
                cols = slice(side * LANES, (side + 1) * LANES)
                bd[k, 0:HEAD, cols] = jnp.where(lane < HEAD, both, 0.0).astype(BF16)
                bd[k, HEAD:LANES, cols] = jnp.where(lane < HEAD, 0.0, both).astype(BF16)
        soft[...] = log1p_of_exp(-lrate[...]) * (-SHARPNESS)
        shift_t[...] = shift[...].T

    def normalize(first, last):
        def body(i, carry):
            at = pl.ds(pl.multiple_of(i * REACH, REACH), REACH)
            x = tok[at, :].astype(F32)
            mean = jnp.sum(x * x, axis=1, keepdims=True) * (1.0 / depth)
            keep = jnp.where(jnp.logical_and(i == 0, sp == 0), 0.0, 1.0)
            nrm[at, :] = (x * lax.rsqrt(mean + EPSILON) * gain[...] * keep).astype(BF16)
            return carry
        lax.fori_loop(first, last, body, 0, unroll=3)

    def project(first, width):
        weight = w[:, :, :, first:first + width].reshape(depth, width)
        result = jnp.dot(nrm[...], weight, preferred_element_type=F32)
        proj[:, first:first + width] = result.astype(BF16).astype(F32)

    def gates(begin, end):
        low = lax.broadcasted_iota(jnp.int32, (seg, LANES), 1) < HEAD

        def body(i, carry):
            first = pl.multiple_of(i * seg, seg)
            at = pl.ds(first, seg)
            for k in range(rnn // LANES):
                cols = slice(k * LANES, (k + 1) * LANES)
                v = proj[pl.ds(first, seg + REACH), cols]
                conv = taps[0:1, cols] * v[13:13 + seg]
                for tap in (1, 2, 3):
                    conv = conv + taps[tap:tap + 1, cols] * v[13 + tap:13 + tap + seg]
                conv = conv.astype(BF16)
                terms = jnp.dot(conv, bd[k], preferred_element_type=F32)
                rate = jax.nn.sigmoid(terms[:, :LANES])
                entry = jax.nn.sigmoid(terms[:, LANES:])
                shifts = jnp.where(
                    low, shift_t[at, 2 * k:2 * k + 1], shift_t[at, 2 * k + 1:2 * k + 2]
                )
                log_decay = rate * soft[0:1, cols] + shifts
                put = pl.ds(pl.multiple_of(i * PITCH, 8), seg)
                decay = jnp.exp(log_decay)
                aa[k, put, :] = decay
                bb[k, put, :] = (
                    jnp.sqrt(one_minus_square(decay, log_decay)) * entry * conv.astype(F32)
                )
            return carry
        lax.fori_loop(begin, end, body, 0)

    def scan():
        tiles = range(rnn // LANES)

        def body(j, carry):
            at = pl.ds(j, SEGMENTS, stride=PITCH)
            result = []
            for k in tiles:
                decay, state = carry[k]
                a, b = aa[k, at, :], bb[k, at, :]
                decay = decay * a
                state = a * state + b
                aa[k, at, :] = decay
                bb[k, at, :] = state
                result.append((decay, state))
            return tuple(result)
        start = (jnp.ones((SEGMENTS, LANES), F32), jnp.zeros((SEGMENTS, LANES), F32))
        for k, (decay, state) in enumerate(lax.fori_loop(0, seg, body, (start,) * len(tiles))):
            ends_a[:, k * LANES:(k + 1) * LANES] = decay
            ends_b[:, k * LANES:(k + 1) * LANES] = state
        total_a, total_b = jnp.ones((1, rnn), F32), jnp.zeros((1, rnn), F32)
        for s in range(SEGMENTS):
            enter[s, :, 0:rnn] = total_a
            enter[s, :, rnn:] = total_b
            a, b = ends_a[s:s + 1, :], ends_b[s:s + 1, :]
            total_a, total_b = total_a * a, a * total_b + b
        ybuf[y, :, 0:rnn] = total_a
        ybuf[y, :, rnn:] = total_b

    def sums_to_others(buf, home, n, sem, target):
        for k in range(1, n):
            pltpu.make_async_remote_copy(
                src_ref=buf.at[home], dst_ref=buf.at[home], send_sem=sem.at[0],
                recv_sem=sem.at[1], device_id={"sp": target(k)}, device_id_type=MESH,
            ).start()

    def chained(buf, n, home):
        whole = before = (jnp.ones((1, rnn), F32), jnp.zeros((1, rnn), F32))
        for s in range(n):
            a, b = buf[s, :, 0:rnn], buf[s, :, rnn:]
            before = tuple(jnp.where(s == home, new, old) for new, old in zip(whole, before))
            whole = (whole[0] * a, a * whole[1] + b)
        return whole, before

    def turned(first):
        return pl.ds(pl.multiple_of(lax.rem(first + (1 - tp) * half, rows), REACH), seg)

    def pool():
        def body(i, carry):
            first = pl.multiple_of(i * seg, seg)
            at = turned(first)
            place = sp * rows + first + lax.broadcasted_iota(jnp.int32, (seg, LANES), 0)
            for g in (0, 1):
                x = proj[pl.ds(first, seg + REACH), POOL + g * LANES:POOL + (g + 1) * LANES]
                near = x + pltpu.roll(x, 1, 0)
                if g == 1:
                    near = near + pltpu.roll(near, 2, 0)
                far = near
                for width in ((2, 4) if g == 0 else (4, 8)):
                    far = far + pltpu.roll(far, width, 0)
                window = jnp.where(tp == 0, 2 << g, 8 << g)
                summed = jnp.where(tp == 0, near, far)[REACH:]
                counts = jnp.minimum(place + 1, window).astype(F32)
                pooled = (summed / counts - x[REACH:]).astype(BF16)
                mixed = jnp.dot(pooled, pmix[g], preferred_element_type=F32)
                cols = slice(g * LANES, (g + 1) * LANES)
                acts[at, rnn + g * LANES:rnn + (g + 1) * LANES] = (
                    mixed * avg[0:1, cols]
                ).astype(BF16)
            return carry
        lax.fori_loop(0, SEGMENTS, body, 0)

    def gelu():
        scale = math.sqrt(2.0 / math.pi)

        def body(i, carry):
            at = pl.ds(pl.multiple_of(REACH + i * seg, REACH), seg)
            cols = slice(GATE, POOL)
            v = proj[at, cols]
            proj[at, cols] = v * (0.5 * (1.0 + jnp.tanh(scale * (v + 0.044715 * (v * v * v)))))
            return carry
        lax.fori_loop(0, SEGMENTS, body, 0)

    def carry_in():
        _, rows_before = chained(zbuf, nz, z)
        _, in_row = chained(ybuf, ny, y)
        entry = rows_before[0] * init[...] + rows_before[1]
        carried[...] = in_row[0] * entry + in_row[1]

    def row_total():
        whole, _ = chained(ybuf, ny, y)
        zbuf[z, :, 0:rnn] = whole[0]
        zbuf[z, :, rnn:] = whole[1]

    def finish():
        def body(i, carry):
            first = pl.multiple_of(i * seg, seg)
            at = pl.ds(pl.multiple_of(i * PITCH, 8), seg)
            put = turned(first)
            begin = enter[i, :, 0:rnn] * carried[...] + enter[i, :, rnn:]
            for k in range(rnn // LANES):
                cols = slice(k * LANES, (k + 1) * LANES)
                state = bb[k, at, :] + aa[k, at, :] * begin[:, cols]
                gate = proj[pl.ds(pl.multiple_of(REACH + first, REACH), seg),
                            GATE + k * LANES:GATE + (k + 1) * LANES]
                acts[put, cols] = (gate * state).astype(BF16)
            return carry
        lax.fori_loop(0, SEGMENTS, body, 0)

    features = ny * w.shape[2]

    def columns(n):
        return pl.ds(pl.multiple_of(n * features, LANES), features)

    def part_copy(n):
        return pltpu.make_async_remote_copy(
            src_ref=psend.at[n], dst_ref=precv.at[:, columns(n)], send_sem=part_send,
            recv_sem=part_recv, device_id={"tp": 1 - tp}, device_id_type=MESH,
        )

    def products():
        def body(n, carry):
            weight = w[pl.ds(2 * n, 2), :, :, OUT:PACKED].reshape(2 * features, PACKED - OUT)
            result = lax.dot_general(
                acts[...], weight, (((1,), (1,)), ((), ())), preferred_element_type=F32
            )
            for side in (0, 1):
                part = result[:, side * features:(side + 1) * features]
                psend[2 * n + side] = part[:half].astype(BF16)
                part_copy(2 * n + side).start()
                own[:, columns(2 * n + side)] = part[half:]
            return carry
        lax.fori_loop(0, nz // 2, body, 0)

    def totals():
        wait_for(precv, part_recv)

    copies = {"pair": (None, 0, ()), "halo": (None, 0, ("pair", "own"))}
    copies.update({"y_sums": (None, 0, ("scan",)), "z_sums": (None, 0, ("row_total",))})
    copies.update(table)
    blocks = (rows + REACH) // REACH
    cuts = [blocks * k // 4 // 3 * 3 for k in range(4)] + [blocks]
    normed = tuple(f"norm{k}" for k in range(4))
    pieces = {"own": (0.0, own_tokens.wait, ()), "prepare": (0.3, prepare, ())}
    for k in range(4):
        pieces[normed[k]] = (
            0.8, functools.partial(normalize, cuts[k], cuts[k + 1]), ("halo",)
        )
    pieces["value"] = (
        1.4, functools.partial(project, VALUE, GATE), complete["value"] + normed
    )
    for k in range(4):
        pieces[f"gates{k}"] = (
            0.65, functools.partial(gates, 2 * k, 2 * k + 2), ("value", "prepare")
        )
    pieces["scan"] = (0.9, scan, tuple(f"gates{k}" for k in range(4)))
    pieces["row_total"] = (0.1, row_total, ("y_sums",))
    pieces["carry_in"] = (0.1, carry_in, ("z_sums",))
    pieces["gate"] = (
        1.4, functools.partial(project, GATE, POOL - GATE), complete["gate"] + normed
    )
    pieces["project_pool"] = (0.8, functools.partial(project, POOL, OUT - POOL), complete["pool"] + normed)
    pieces["gelu"] = (0.4, gelu, ("gate",))
    pieces["pool"] = (1.4, pool, ("project_pool", "prepare"))
    pieces["finish"] = (0.3, finish, ("carry_in", "gelu"))
    pieces["products"] = (2.5, products, ("finish", "pool") + complete["out"])
    pieces["totals"] = (1.0, totals, ("products",))

    def start(key):
        if key == "pair":
            pair.start()
        elif key == "halo":
            halo.start()
        elif key == "y_sums":
            sums_to_others(ybuf, y, ny, y_sem, at_y)
        elif key == "z_sums":
            sums_to_others(zbuf, z, nz, z_sem, at_z)
        else:
            gather_copy(key).start()

    def wait(group):
        if group == "pair":
            pair.wait_recv()
        elif group == "halo":
            halo.wait_recv()
        elif group == "y_sums":
            wait_for(ybuf.at[0:ny - 1], y_sem.at[1])
        elif group == "z_sums":
            wait_for(zbuf.at[0:nz - 1], z_sem.at[1])
        else:
            arrived(group)

    waited = set()

    def settle(keys):
        for key in keys:
            group = recvs.get(key, key)
            if key in copies and group not in waited:
                waited.add(group)
                wait(group)

    for key in planned(copies, {k: (v[0], v[2]) for k, v in pieces.items()}):
        if key in copies:
            settle(copies[key][-1])
            start(key)
        else:
            settle(pieces[key][-1])
            pieces[key][1]()
    settle(copies)

    for group, k in send_at.items():
        wait_for(block_of(*group, "all"), ring_send.at[k])
    pair.wait_send()
    halo.wait_send()
    wait_for(ybuf.at[0:ny - 1], y_sem.at[0])
    wait_for(zbuf.at[0:nz - 1], z_sem.at[0])
    wait_for(psend, part_send)


def shards(ny, nz, tokens, norm_gain, pool_in, gate_in, value_in, pool_mix, averaging_factor,
           conv_taps, rate_mix, input_mix, log_rate, decay_shift, initial_state, out_pool,
           out_rnn):
    half, depth = tokens.shape
    rows = 2 * half
    rnn = log_rate.shape[0]
    lines = pool_in.shape[0]
    features = ny * lines
    sends, recvs = semaphores_of(transfers_of(ny, nz, lines)[0], ny, nz)
    dma = pltpu.SemaphoreType.DMA
    vmem = pltpu.VMEM
    scratch = [
        vmem((nz, ny, lines, PACKED), BF16),
        vmem((rows + REACH, depth), BF16),
        vmem((rows + REACH, depth), BF16),
        vmem((rows + REACH, OUT), F32),
        vmem((rnn // LANES, SEGMENTS * PITCH, LANES), F32),
        vmem((rnn // LANES, SEGMENTS * PITCH, LANES), F32),
        vmem((rows, PACKED - OUT), BF16),
        vmem((rows, rnn // HEAD), F32),
        vmem((1, depth), F32),
        vmem(pool_mix.shape, BF16),
        vmem((1, 2 * LANES), F32),
        vmem(conv_taps.shape, F32),
        vmem(rate_mix.shape, BF16),
        vmem(input_mix.shape, BF16),
        vmem((1, rnn), F32),
        vmem(decay_shift.shape, F32),
        vmem((1, rnn), F32),
        vmem((rnn // LANES, LANES, 2 * LANES), BF16),
        vmem((1, rnn), F32),
        vmem((SEGMENTS, rnn), F32),
        vmem((SEGMENTS, rnn), F32),
        vmem((SEGMENTS, 1, 2 * rnn), F32),
        vmem((1, rnn), F32),
        vmem((ny, 1, 2 * rnn), F32),
        vmem((nz, 1, 2 * rnn), F32),
        vmem((nz, half, features), BF16),
        dma((11,)),
        dma((len(set(sends.values())),)),
        dma((len(set(recvs.values())),)),
        dma, dma, dma, dma,
        dma((2,)), dma((2,)), dma, dma,
    ]
    anywhere = pl.BlockSpec(memory_space=pl.ANY)
    own, theirs = pl.pallas_call(
        functools.partial(kernel, ny, nz),
        out_shape=(vmem((half, depth), F32), vmem((half, depth), BF16)),
        in_specs=[anywhere] * 15,
        out_specs=(pl.BlockSpec(memory_space=vmem),) * 2,
        scratch_shapes=scratch,
        compiler_params=pltpu.CompilerParams(
            collective_id=0, has_side_effects=True, vmem_limit_bytes=56 * 1024 * 1024
        ),
        name="layer",
    )(tokens, norm_gain[None], pool_in, gate_in, value_in, pool_mix, averaging_factor[None],
      conv_taps, rate_mix, input_mix, log_rate[None], decay_shift, initial_state[None], out_pool,
      out_rnn)
    return (own + theirs.astype(F32)).astype(BF16)


def grid_of(count):
    ny = 1
    while ny * ny < count:
        ny *= 2
    return ny, count // ny


def solution(mesh):
    ny, nz = grid_of(mesh.shape["sp"])
    placed = (
        P(("fs", "sp", "tp"), None),
        P(),
        P("sp", "tp"),
        P("sp", "tp"),
        P("sp", "tp"),
        P("tp", None, None),
        P("tp"),
        P(None, "tp"),
        P("tp", None, None),
        P("tp", None, None),
        P("tp"),
        P(("fs", "tp"), "sp"),
        P(("fs", "tp")),
        P("sp", "tp"),
        P("sp", "tp"),
    )
    return jax.shard_map(
        functools.partial(shards, ny, nz), mesh=mesh, in_specs=placed,
        out_specs=P(("fs", "sp", "tp"), None), check_vma=False,
    )
```
